256 devices in a mesh: grp: 2 (over y), ep: 32 (over z, core), tp: 4 (over x).
Axes of the slice: x: 4, y: 2, z: 16, core: 2. Of those that a mesh axis runs over, the one named last changes fastest.
The devices are a block of a 4x16x16 slice.
Arguments:
- query: bfloat16 [65536, 1024], P(('grp', 'ep'), 'tp'), parts along dimension 0, may hold values from -6 to 6
- forget_gate_logits: bfloat16 [65536, 1024], P(('grp', 'ep'), 'tp'), parts along dimension 0, may hold values from -8 to 8
- value: bfloat16 [65536, 1024], P(('grp', 'ep'), 'tp'), parts along dimension 0, may hold values from -6 to 6
- forget_lower_margin: float32 [2, 1024], P(None, 'tp'), may hold values from -30 to -2
- position_log_decay: float32 [8, 65536], P('tp', ('grp', 'ep')), parts along dimension 1, may hold values from -1.5 to 0
- head_norm_gain: float32 [128], replicated, may hold values from 0.1 to 1.9
- mixer_output_weight: bfloat16 [1024, 2048], P('tp'), may hold values from -0.1875 to 0.1875
- second_batch_tokens: bfloat16 [32768, 2048], P(('grp', 'ep', 'tp')), parts along dimension 0, may hold values from -60 to 60
- expert_norm_gain: float32 [2048], replicated, may hold values from 0.1 to 1.9
- routes: int32 [32768, 2], P(('grp', 'ep', 'tp')), parts along dimension 0, may hold values from 0 to 31, all different within a row; in each aligned block of 128 rows (0 to 127, 128 to 255, ...) at most 12 rows name the same one
- chosen_expert_weight: float32 [32768, 2], P(('grp', 'ep', 'tp')), parts along dimension 0, may hold values from 0.2 to 1
- gate_weight: bfloat16 [32, 2048, 2048], P('ep', None, 'tp'), may hold values from -0.3125 to 0.3125
- up_weight: bfloat16 [32, 2048, 2048], P('ep', None, 'tp'), may hold values from -0.3125 to 0.3125
- down_weight: bfloat16 [32, 2048, 2048], P('ep', 'tp'), may hold values from -0.02734375 to 0.02734375
Outputs:
- first_mixer_output: bfloat16 [65536, 2048], P(('grp', 'ep', 'tp')), parts along dimension 0
- moe_out: bfloat16 [32768, 2048], P(('grp', 'ep', 'tp')), parts along dimension 0
The draws below stay inside these ranges and needn't reach their ends.
There are 2 independent parts, one for each index of `grp`. The reference program is written for one: setup_inputs(seed, part) draws one part's arguments, and reference() takes and returns one part's arrays. A program takes and returns all parts, laid end to end along the dimension named above; an argument that names none is the same for every part. Nothing has to cross between parts.
Inputs may be any that keep to these rules, and one draw needn't show every extreme that they name: `routes`: each row names 2 different experts. Among the rows of one device no expert is named by more than 12 rows, and in every draw some expert is named by exactly 12 rows of some device.
All inputs are finite; a program needn't handle non-finite values.
Results may differ from the reference program's by a relative error of at most 0.015.
Values may be sent and summed in bfloat16 or wider, within the bound.
No kernel may reach another device: no remote copies, remote signals or barrier semaphores. Data moves between devices by JAX's collectives and lax.ppermute only.
A program may use at most 128 MiB of HBM per device.

```python
import math
import jax
import jax.numpy as jnp
import numpy as np
from jax import lax

D = 2048
RECURRENT_HEADS = 8
HEAD_CHANNELS = 128
FF = 2048
TOPK = 2
BLK = 128
ROWS = 1024
TOK_DEV = 128
SEQUENCE_TOKENS = 32768
MOE_TOKENS = 16384
EXPERTS = 32
CAP = 12
HEAD_GROUP = 2
FF_GROUP = 512
N_EP = 32
N_TP = 4


def draw_forget_lower_margin(key, part):
    key = jax.random.fold_in(key, 101)
    pick_key, fast_key, slow_key = jax.random.split(key, 3)
    share = 0.5
    slow_heads = jax.random.uniform(pick_key, (2, RECURRENT_HEADS, 1)) < share
    fast_gap = jnp.log(jax.random.uniform(fast_key, (2, RECURRENT_HEADS, HEAD_CHANNELS), minval=0.02, maxval=0.06))
    slow_gap = jax.random.uniform(slow_key, (2, RECURRENT_HEADS, HEAD_CHANNELS), minval=jnp.log(0.1), maxval=jnp.log(0.4)) - jnp.log(float(SEQUENCE_TOKENS))
    chosen = jnp.where(slow_heads, slow_gap, fast_gap)
    return chosen.reshape(2, RECURRENT_HEADS * HEAD_CHANNELS).astype(jnp.float32)


def draw_position_log_decay(key, part):
    key = jax.random.fold_in(key, 202)
    rate_key, place_key, size_key = jax.random.split(key, 3)
    blocks = SEQUENCE_TOKENS // ROWS
    rates = jnp.exp(jax.random.uniform(rate_key, (RECURRENT_HEADS, blocks, 1), minval=jnp.log(0.15), maxval=jnp.log(0.6)))
    steady = jnp.broadcast_to(rates / SEQUENCE_TOKENS, (RECURRENT_HEADS, blocks, ROWS)).reshape(RECURRENT_HEADS, SEQUENCE_TOKENS)
    places = jax.random.randint(place_key, (RECURRENT_HEADS, 2), 0, SEQUENCE_TOKENS)
    sizes = jax.random.uniform(size_key, (RECURRENT_HEADS, 2), minval=0.22, maxval=0.69)
    positions = jnp.arange(SEQUENCE_TOKENS, dtype=jnp.int32)
    hits = jnp.sum(jnp.where(positions[None, None, :] == places[:, :, None], sizes[:, :, None], 0.0), axis=1)
    return (-steady - hits).astype(jnp.float32)


def draw_second_batch_tokens(key, part):
    key = jax.random.fold_in(key, 303)
    base_key, row_key, column_key = jax.random.split(key, 3)
    base = jnp.clip(jax.random.normal(base_key, (MOE_TOKENS, D)), -5.0, 5.0)
    row_scale = jnp.exp(jax.random.uniform(row_key, (MOE_TOKENS, 1), minval=jnp.log(0.3), maxval=jnp.log(3.0)))
    column_scale = jnp.exp(jax.random.uniform(column_key, (1, D), minval=jnp.log(0.4), maxval=jnp.log(4.0)))
    return (base * row_scale * column_scale).astype(jnp.bfloat16)


def level_of(own_key, dims, pieces, smallest, largest):
    factor_of, own = 1.0, jax.random.fold_in(own_key, 6)
    for axis_at, blocks in pieces:
        steps = jnp.exp(jax.random.uniform(jax.random.fold_in(own, axis_at), (blocks,), jnp.float32, smallest / len(pieces), largest / len(pieces)))
        factor_of = factor_of * jnp.repeat(steps, dims[axis_at] // blocks).reshape([-1 if axis == axis_at else 1 for axis in range(len(dims))])
    return factor_of


def routed_block(stream_key, own, number, rows, number_of, top, reach, skew):
    ranking = jax.random.permutation(stream_key, number_of)
    heavy_load, ordinary = load_shares(number_of, rows * top, reach, skew, True), load_shares(number_of, rows * top, reach, skew, False)
    places = jnp.arange(number_of)

    def named(tallies, turn):
        used = int((tallies > 0).sum())
        fixed = max(1, used // 4)
        shifted = fixed + (places - fixed + turn * (used - fixed)) % max(1, number_of - fixed)
        return jnp.zeros((number_of,), jnp.int32).at[ranking[jnp.where(places < fixed, places, shifted)]].set(jnp.asarray(tallies, jnp.int32))

    tallies = jnp.where(number % 4 == 0, named(heavy_load, number // 4), named(ordinary, number - number // 4 - 1))
    mixed = jax.random.permutation(jax.random.fold_in(own, 3), number_of)
    giver, sink = mixed[0:number_of // 2 * 2:2], mixed[1:number_of // 2 * 2:2]
    margin = jnp.minimum(tallies[giver] - 1, reach - tallies[sink]) // 2
    margin = jnp.where((giver == ranking[0]) | (sink == ranking[0]) | (tallies[sink] == 0), 0, jnp.maximum(margin, 0))
    shifted = jax.random.randint(jax.random.fold_in(own, 4), (number_of // 2,), 0, 1 << 20) % (margin + 1)
    tallies = tallies.at[giver].add(-shifted).at[sink].add(shifted)
    members = jnp.searchsorted(jnp.cumsum(tallies), jnp.arange(rows * top), side="right").astype(jnp.int32)
    grid = members.reshape(top, rows).T
    grid = grid[jax.random.permutation(jax.random.fold_in(own, 1), rows)]
    turn = jax.random.randint(jax.random.fold_in(own, 2), (rows, 1), 0, top)
    return jnp.take_along_axis(grid, (jnp.arange(top)[None, :] + turn) % top, axis=1)


def load_shares(count, total, limit, slope, full):
    loads = [(1 << 20) // math.isqrt(grade ** slope) + 1 for grade in range(1, count + 1)]
    largest = limit if full else min(limit, max(-(-total // count), total * loads[0] // sum(loads)))
    least = 1 if total - largest >= count - 1 else 0
    given, surplus = [largest] + [least] * (count - 1), total - largest - least * (count - 1)
    while surplus > 0:
        free = [i for i in range(1, count) if given[i] < largest] or [i for i in range(1, count) if given[i] < limit]
        whole, remaining = sum([loads[i] for i in free]), surplus
        for i in free:
            more = min(limit - given[i], max(1, remaining * loads[i] // whole), surplus)
            given[i] = given[i] + more
            surplus = surplus - more
    return np.array(given)


def noise(stream_key, dims, spread, most, cuts=(), kind=jnp.bfloat16):
    loudness = level_of(stream_key, dims, cuts, -0.22, 0.18) if cuts else 1.0
    values = jax.random.normal(stream_key, dims, jnp.float32) * spread * loudness
    return jnp.minimum(jnp.maximum(values, -most), most).astype(kind)


def setup_inputs(seed: int = 0, part: int = 0) -> dict:
    seeds = jax.random.split(jax.random.key(seed), 15)
    own_keys = jax.random.split(jax.random.fold_in(seeds[14], part), 15)
    query = noise(own_keys[0], (SEQUENCE_TOKENS, RECURRENT_HEADS * HEAD_CHANNELS), 1.0, 6.0, ((0, 32), (1, 4)))
    forget_gate_logits = noise(own_keys[1], (SEQUENCE_TOKENS, RECURRENT_HEADS * HEAD_CHANNELS), 1.5, 8.0, ((0, 32), (1, 4)))
    value = noise(own_keys[2], (SEQUENCE_TOKENS, RECURRENT_HEADS * HEAD_CHANNELS), 1.0, 6.0, ((0, 32), (1, 4)))
    forget_lower_margin = draw_forget_lower_margin(jax.random.fold_in(seeds[14], 71), part)
    position_log_decay = draw_position_log_decay(jax.random.fold_in(jax.random.fold_in(seeds[14], part), 71), part)
    head_norm_gain = jnp.clip(1.0 + 0.18 * jax.random.normal(seeds[5], (HEAD_CHANNELS,), jnp.float32), 0.1, 1.9)
    mixer_output_weight = noise(seeds[6], (RECURRENT_HEADS * HEAD_CHANNELS, D), (RECURRENT_HEADS * HEAD_CHANNELS) ** -0.5, 0.1875, ((0, 4),))
    second_batch_tokens = draw_second_batch_tokens(jax.random.fold_in(jax.random.fold_in(seeds[14], part), 71), part)
    expert_norm_gain = jnp.clip(1.0 + 0.18 * jax.random.normal(seeds[8], (D,), jnp.float32), 0.1, 1.9)
    routes_keys = jax.random.split(jax.random.fold_in(own_keys[9], 1), MOE_TOKENS // TOK_DEV)
    routes_turns = jax.random.permutation(jax.random.fold_in(own_keys[9], 3), MOE_TOKENS // TOK_DEV)
    routes = jax.vmap(lambda own, number: routed_block(jax.random.fold_in(own_keys[9], 2), own, number, TOK_DEV, EXPERTS, TOPK, CAP, 2))(routes_keys, routes_turns).reshape((MOE_TOKENS, TOPK))
    chosen_expert_weight = jnp.clip(0.2 + 0.8 * jax.random.uniform(own_keys[10], (MOE_TOKENS, TOPK), jnp.float32) ** level_of(own_keys[10], (MOE_TOKENS, TOPK), ((0, 128),), -0.2, 0.2), 0.2, 1.0)
    gate_weight = noise(seeds[11], (EXPERTS, D, FF), (D // 6) ** -0.5, 0.3125, ((0, 32), (2, 4)))
    up_weight = noise(seeds[12], (EXPERTS, D, FF), (D // 6) ** -0.5, 0.3125, ((0, 32), (2, 4)))
    down_weight = noise(seeds[13], (EXPERTS, FF, D), (25 * FF) ** -0.5, 0.02734375, ((0, 32), (1, 4)))
    return {"query": query, "forget_gate_logits": forget_gate_logits, "value": value, "forget_lower_margin": forget_lower_margin, "position_log_decay": position_log_decay, "head_norm_gain": head_norm_gain, "mixer_output_weight": mixer_output_weight, "second_batch_tokens": second_batch_tokens, "expert_norm_gain": expert_norm_gain, "routes": routes, "chosen_expert_weight": chosen_expert_weight, "gate_weight": gate_weight, "up_weight": up_weight, "down_weight": down_weight}


NORM_EPS = 1e-06
CLAMP_LIMIT = 7.0
SIGMOID_SCALE = 1.702
PRECISE = lax.Precision.HIGHEST

def clamped_unit(gate_pre, up_pre):
    gate_pre = jnp.minimum(gate_pre, CLAMP_LIMIT)
    up_pre = jnp.clip(up_pre, -CLAMP_LIMIT, CLAMP_LIMIT)
    return (up_pre + 1.0) * gate_pre * jax.nn.sigmoid(SIGMOID_SCALE * gate_pre)

def block_recurrence(queries, ending_state, values, forget_log_rates):
    sequence_length, number_of_heads, channels = queries.shape
    nblocks = sequence_length // BLK

    def to_blocks(array):
        return array.reshape(nblocks, BLK, number_of_heads, array.shape[-1])
    query_blocks = to_blocks(queries)
    key_blocks = to_blocks(ending_state)
    value_blocks = to_blocks(values)
    cumul = jnp.cumsum(to_blocks(forget_log_rates), axis=1)
    block_last = cumul[:, -1]
    query_in = query_blocks * jnp.exp(cumul)
    key_in = key_blocks * jnp.exp(-cumul)
    key_state = key_blocks * jnp.exp(block_last[:, None] - cumul)
    lower = jnp.tril(jnp.ones((BLK, BLK), jnp.float32))
    scores = jnp.einsum('nchd,nshd->nhcs', query_in, key_in, precision=PRECISE) * lower
    inner = jnp.einsum('nhcs,nshv->nchv', scores, value_blocks, precision=PRECISE)
    increments = jnp.einsum('nshd,nshv->nhdv', key_state, value_blocks, precision=PRECISE)

    def advance(state, inputs):
        decay, increment = inputs
        return (state * decay[..., None] + increment, state)
    initial = jnp.zeros((number_of_heads, channels, values.shape[-1]), jnp.float32)
    final_state, before = lax.scan(advance, initial, (jnp.exp(block_last), increments))
    outer = jnp.einsum('nchd,nhdv->nchv', query_in, before, precision=PRECISE)
    return (inner + outer).reshape(sequence_length, number_of_heads, values.shape[-1])

def token_mixer(query, forget_gate_logits, value, forget_lower_margin, position_log_decay, head_norm_gain, mixer_output_weight):
    queries = jax.nn.silu(query.astype(jnp.float32)).reshape(SEQUENCE_TOKENS, RECURRENT_HEADS, HEAD_CHANNELS) * HEAD_CHANNELS ** (-0.5)
    values = value.astype(jnp.float32).reshape(SEQUENCE_TOKENS, RECURRENT_HEADS, HEAD_CHANNELS)
    shutting = jax.nn.sigmoid(-forget_gate_logits.astype(jnp.float32))
    decay_spikes = jnp.transpose(position_log_decay)[:, :, None]
    mix = jnp.zeros((SEQUENCE_TOKENS, RECURRENT_HEADS, HEAD_CHANNELS), jnp.float32)
    for direction in range(2):
        ending_state = jnp.exp(forget_lower_margin[direction])[None, :] * shutting
        forget_log_rates = jnp.log1p(-ending_state).reshape(SEQUENCE_TOKENS, RECURRENT_HEADS, HEAD_CHANNELS) + decay_spikes
        ending_state = ending_state.reshape(SEQUENCE_TOKENS, RECURRENT_HEADS, HEAD_CHANNELS)
        if direction == 0:
            mix = mix + block_recurrence(queries, ending_state, values, forget_log_rates)
        else:
            turned = block_recurrence(jnp.flip(queries, 0), jnp.flip(ending_state, 0), jnp.flip(values, 0), jnp.flip(forget_log_rates, 0))
            mix = mix + jnp.flip(turned, 0)
    scaled = mix * lax.rsqrt(lax.optimization_barrier(jnp.mean(mix * mix, axis=-1, keepdims=True)) + NORM_EPS) * head_norm_gain
    head_outputs = scaled.reshape(SEQUENCE_TOKENS, RECURRENT_HEADS * HEAD_CHANNELS).astype(jnp.bfloat16)
    group_width = HEAD_GROUP * HEAD_CHANNELS
    summed = jnp.zeros((SEQUENCE_TOKENS, D), jnp.float32)
    for group in range(N_TP):
        part_sum = jnp.dot(head_outputs[:, group * group_width:(group + 1) * group_width], mixer_output_weight[group * group_width:(group + 1) * group_width], preferred_element_type=jnp.float32).astype(jnp.bfloat16)
        summed = summed + part_sum.astype(jnp.float32)
    return summed.astype(jnp.bfloat16)

def experts(second_batch_tokens, expert_norm_gain, routes, chosen_expert_weight, gate_weight, up_weight, down_weight):
    tokens_f = second_batch_tokens.astype(jnp.float32)
    normed = (tokens_f * lax.rsqrt(lax.optimization_barrier(jnp.mean(tokens_f * tokens_f, axis=-1, keepdims=True)) + NORM_EPS) * expert_norm_gain).astype(jnp.bfloat16)
    count = normed.shape[0]
    padded = jnp.concatenate([normed, jnp.zeros((1, D), jnp.bfloat16)], axis=0)
    flat_routes = routes.reshape(-1)
    scales_all = jnp.concatenate([chosen_expert_weight.reshape(-1), jnp.zeros((1,), jnp.float32)])
    most_rows = CAP * N_EP * N_TP

    def one_expert(running, expert):
        positions, = jnp.nonzero(flat_routes == expert, size=most_rows, fill_value=count * TOPK)
        positions = positions.astype(jnp.int32)
        owners = positions // TOPK
        picked_rows = padded[owners]
        scales = scales_all[positions]
        gate_pre = jnp.dot(picked_rows, gate_weight[expert], preferred_element_type=jnp.float32)
        up_pre = jnp.dot(picked_rows, up_weight[expert], preferred_element_type=jnp.float32)
        hidden = clamped_unit(gate_pre, up_pre).astype(jnp.bfloat16)
        result = jnp.zeros((most_rows, D), jnp.float32)
        for group in range(N_TP):
            part_sum = jnp.dot(hidden[:, group * FF_GROUP:(group + 1) * FF_GROUP], down_weight[expert, group * FF_GROUP:(group + 1) * FF_GROUP], preferred_element_type=jnp.float32).astype(jnp.bfloat16)
            result = result + part_sum.astype(jnp.float32)
        rounded = lax.optimization_barrier(result.astype(jnp.bfloat16)).astype(jnp.float32)
        running = running.at[owners].add(scales[:, None] * rounded)
        return (running, None)
    start_sum = jnp.zeros((count + 1, D), jnp.float32)
    total_sum, _ = lax.scan(one_expert, start_sum, jnp.arange(EXPERTS, dtype=jnp.int32))
    return total_sum[:count].astype(jnp.bfloat16)

def reference(query, forget_gate_logits, value, forget_lower_margin, position_log_decay, head_norm_gain, mixer_output_weight, second_batch_tokens, expert_norm_gain, routes, chosen_expert_weight, gate_weight, up_weight, down_weight):
    first_mixer_output = token_mixer(query, forget_gate_logits, value, forget_lower_margin, position_log_decay, head_norm_gain, mixer_output_weight)
    moe_out = experts(second_batch_tokens, expert_norm_gain, routes, chosen_expert_weight, gate_weight, up_weight, down_weight)
    return (first_mixer_output, moe_out)
```

```python
import functools

import jax
import jax.numpy as jnp
from jax import lax
from jax.experimental import pallas as pl
from jax.experimental.pallas import tpu as pltpu
from jax.sharding import Mesh
from jax.sharding import PartitionSpec as P


HEAD_CHANNELS = 128
BLK = 128
STATE_ROWS = HEAD_CHANNELS + 16
EP = ("ep_0", "ep_1")
GRP_EP = ("grp", "ep_0", "ep_1")
GRP_EP_TP = ("grp", "ep_0", "ep_1", "tp")
TILE = 8

NORM_EPS = 1e-06
CLAMP_LIMIT = 7.0
SIGMOID_SCALE = 1.702

F32 = jnp.float32
BF16 = jnp.bfloat16


def mm(a, b, lhs_dim, rhs_dim):
    return lax.dot_general(
        a, b, (((lhs_dim,), (rhs_dim,)), ((), ())), preferred_element_type=F32
    )


def pieces_of(x):
    high = x.astype(BF16)
    rest = x - high.astype(F32)
    middle = rest.astype(BF16)
    low = (rest - middle.astype(F32)).astype(BF16)
    return high, middle, low


def summed_along(triangle, x):
    return sum(mm(triangle, piece, 1, 0) for piece in pieces_of(x))


def triangle_of(size, keep):
    rows = lax.broadcasted_iota(jnp.int32, (size, size), 0)
    columns = lax.broadcasted_iota(jnp.int32, (size, size), 1)
    return keep(rows, columns)


def block_gates(logits, margin, decay_row, triangle):
    closing = jnp.exp(margin) * jax.nn.sigmoid(-logits.astype(F32))
    spikes = jnp.transpose(jnp.broadcast_to(decay_row, (BLK, BLK)))
    return closing, summed_along(triangle, jnp.log1p(-closing) + spikes)


def advanced(state, total, closing, cumul, values):
    key_state = (closing * jnp.exp(total - cumul)).astype(BF16)
    return state * jnp.exp(total) + mm(values, key_state, 0, 0)


def rows_of(block):
    return pl.ds(pl.multiple_of(block * BLK, BLK), BLK)


def states_kernel(logits_ref, value_ref, margin_ref, decay_ref, state_ref):
    blocks = logits_ref.shape[0] // BLK
    lower = triangle_of(BLK, lambda r, c: r >= c).astype(BF16)
    upper = triangle_of(BLK, lambda r, c: r <= c).astype(BF16)

    def step(i, carry):
        states, logs = [], []
        for d in range(2):
            block = i if d == 0 else blocks - 1 - i
            rows = rows_of(block)
            closing, cumul = block_gates(
                logits_ref[rows, :],
                margin_ref[d : d + 1, :],
                decay_ref[0, :, rows],
                lower if d == 0 else upper,
            )
            total = cumul[BLK - 1 :, :] if d == 0 else cumul[:1, :]
            states.append(advanced(carry[0][d], total, closing, cumul, value_ref[rows, :]))
            logs.append(carry[1][d] + total)
        return tuple(states), tuple(logs)

    zero_state = jnp.zeros((HEAD_CHANNELS, HEAD_CHANNELS), F32)
    zero_log = jnp.zeros((1, HEAD_CHANNELS), F32)
    states, logs = lax.fori_loop(0, blocks, step, ((zero_state,) * 2, (zero_log,) * 2))
    places = lax.broadcasted_iota(jnp.int32, (STATE_ROWS - HEAD_CHANNELS, HEAD_CHANNELS), 0)
    for d in range(2):
        state_ref[0, d, :HEAD_CHANNELS, :] = states[d].astype(BF16)
        tail = jnp.zeros(places.shape, F32)
        for k, piece in enumerate(pieces_of(logs[d])):
            tail = jnp.where(places == k, piece.astype(F32), tail)
        state_ref[0, d, HEAD_CHANNELS:, :] = tail.astype(BF16)


def mixer_states(logits, value, margin, decay):
    tokens, channels = logits.shape
    heads = channels // HEAD_CHANNELS
    return pl.pallas_call(
        states_kernel,
        grid=(heads,),
        in_specs=[
            pl.BlockSpec((tokens, HEAD_CHANNELS), lambda h: (0, h)),
            pl.BlockSpec((tokens, HEAD_CHANNELS), lambda h: (0, h)),
            pl.BlockSpec((2, HEAD_CHANNELS), lambda h: (0, h)),
            pl.BlockSpec((1, 1, tokens), lambda h: (h, 0, 0)),
        ],
        out_specs=pl.BlockSpec((1, 2, STATE_ROWS, HEAD_CHANNELS), lambda h: (h, 0, 0, 0)),
        out_shape=jax.ShapeDtypeStruct((heads, 2, STATE_ROWS, HEAD_CHANNELS), BF16),
        cost_estimate=pl.CostEstimate(
            flops=24 * tokens * channels * BLK, bytes_accessed=5 * tokens * channels, transcendentals=0
        ),
        name="mixer_states",
    )(logits, value, margin, decay.reshape(heads, 1, tokens))


def heads_kernel(
    place_ref, query_ref, logits_ref, value_ref, margin_ref, decay_ref, gain_ref, gathered_ref, out_ref, part_ref
):
    blocks = logits_ref.shape[0] // BLK
    others = gathered_ref.shape[0]
    place = place_ref[0]

    def entering(d):
        def step(i, state):
            j = i if d == 0 else others - 1 - i
            passed = (j < place) if d == 0 else (j > place)
            tail = gathered_ref[j, 0, d, HEAD_CHANNELS:, :].astype(F32)
            decay = jnp.exp(tail[0:1, :] + tail[1:2, :] + tail[2:3, :])
            later = state * decay + gathered_ref[j, 0, d, :HEAD_CHANNELS, :].astype(F32)
            return jnp.where(passed, later, state)

        return lax.fori_loop(0, others, step, jnp.zeros((HEAD_CHANNELS, HEAD_CHANNELS), F32))

    def part(block, state, d):
        rows = rows_of(block)
        keep = triangle_of(BLK, (lambda r, c: r >= c) if d == 0 else (lambda r, c: r <= c))
        values = value_ref[rows, :]
        closing, cumul = block_gates(
            logits_ref[rows, :], margin_ref[d : d + 1, :], decay_ref[0, :, rows], keep.astype(BF16)
        )
        queries = query_ref[rows, :].astype(F32)
        queries = queries * jax.nn.sigmoid(queries) * HEAD_CHANNELS ** (-0.5)
        query_in = (queries * jnp.exp(cumul)).astype(BF16)
        key_in = (closing * jnp.exp(-cumul)).astype(BF16)
        scores = jnp.where(keep, mm(query_in, key_in, 1, 1), 0.0).astype(BF16)
        output = mm(scores, values, 1, 0) + mm(query_in, state.astype(BF16), 1, 1)
        total = cumul[BLK - 1 :, :] if d == 0 else cumul[:1, :]
        return output, advanced(state, total, closing, cumul, values)

    def backward(i, state):
        block = blocks - 1 - i
        output, state = part(block, state, 1)
        part_ref[rows_of(block), :] = output
        return state

    def forward(block, state):
        output, state = part(block, state, 0)
        rows = rows_of(block)
        mix = output + part_ref[rows, :]
        scale = lax.rsqrt(jnp.mean(mix * mix, axis=-1, keepdims=True) + NORM_EPS)
        per = out_ref.shape[2] // BLK
        part_rows = pl.ds(pl.multiple_of((block % per) * BLK, BLK), BLK)
        out_ref[block // per, 0, part_rows, :] = (mix * scale * gain_ref[...]).astype(BF16)
        return state

    lax.fori_loop(0, blocks, backward, entering(1))
    lax.fori_loop(0, blocks, forward, entering(0))


def mixer_heads(place, query, logits, value, margin, decay, gain, gathered, owners):
    tokens, channels = logits.shape
    heads = channels // HEAD_CHANNELS
    others = gathered.shape[0]
    column = pl.BlockSpec((tokens, HEAD_CHANNELS), lambda h, p: (0, h))
    return pl.pallas_call(
        heads_kernel,
        grid_spec=pltpu.PrefetchScalarGridSpec(
            num_scalar_prefetch=1,
            grid=(heads,),
            in_specs=[
                column,
                column,
                column,
                pl.BlockSpec((2, HEAD_CHANNELS), lambda h, p: (0, h)),
                pl.BlockSpec((1, 1, tokens), lambda h, p: (h, 0, 0)),
                pl.BlockSpec((1, HEAD_CHANNELS), lambda h, p: (0, 0)),
                pl.BlockSpec((others, 1, 2, STATE_ROWS, HEAD_CHANNELS), lambda h, p: (0, h, 0, 0, 0)),
            ],
            out_specs=pl.BlockSpec((owners, 1, tokens // owners, HEAD_CHANNELS), lambda h, p: (0, h, 0, 0)),
            scratch_shapes=[pltpu.VMEM((tokens, HEAD_CHANNELS), F32)],
        ),
        out_shape=jax.ShapeDtypeStruct((owners, heads, tokens // owners, HEAD_CHANNELS), BF16),
        cost_estimate=pl.CostEstimate(
            flops=48 * tokens * channels * BLK, bytes_accessed=16 * tokens * channels, transcendentals=0
        ),
        name="mixer_heads",
    )(
        place,
        query,
        logits,
        value,
        margin,
        decay.reshape(heads, 1, tokens),
        gain.reshape(1, HEAD_CHANNELS),
        gathered,
    )


def project_kernel(core_ref, heads_ref, mine_ref, other_ref, out_ref, total_ref):
    core = core_ref[0]
    step = pl.program_id(0)
    part = mm(heads_ref[0, core], mine_ref[0], 1, 0) + mm(heads_ref[0, 1 - core], other_ref[0], 1, 0)

    @pl.when(step == 0)
    def _():
        total_ref[...] = part

    @pl.when(step > 0)
    def _():
        total_ref[...] += part

    @pl.when(step == pl.num_programs(0) - 1)
    def _():
        out_ref[...] = total_ref[...].astype(BF16)


def project(core, heads, mine, other):
    groups, pair, tokens, channels = heads.shape
    features = mine.shape[2]
    weight = pl.BlockSpec((1, channels, features), lambda t, c: (t, 0, 0))
    return pl.pallas_call(
        project_kernel,
        grid_spec=pltpu.PrefetchScalarGridSpec(
            num_scalar_prefetch=1,
            grid=(groups,),
            in_specs=[pl.BlockSpec((1, pair, tokens, channels), lambda t, c: (t, 0, 0, 0)), weight, weight],
            out_specs=pl.BlockSpec((tokens, features), lambda t, c: (0, 0)),
            scratch_shapes=[pltpu.VMEM((tokens, features), F32)],
        ),
        out_shape=jax.ShapeDtypeStruct((tokens, features), BF16),
        cost_estimate=pl.CostEstimate(
            flops=2 * heads.size * features, bytes_accessed=8 * tokens * features, transcendentals=0
        ),
        name="mixer_project",
    )(core, heads, mine, other)


def slots_of(routes, core, experts):
    tokens = routes.shape[0]
    number = lax.broadcasted_iota(jnp.int32, (tokens, experts), 1)
    named = [routes[:, k : k + 1] == number for k in range(routes.shape[1])]
    counts = sum(n.astype(F32) for n in named).astype(BF16)
    earlier = triangle_of(tokens, lambda r, c: r > c).astype(BF16)
    ranking = mm(earlier, counts, 1, 0)
    result = []
    for k, n in enumerate(named):
        slot = jnp.sum(jnp.where(n, ranking, 0.0), axis=1, keepdims=True).astype(jnp.int32)
        expert = routes[:, k : k + 1]
        chip = expert // 2
        far = jnp.where(expert - 2 * chip == core, 0, 1)
        late = slot >= TILE
        block = jnp.where(late, 2 + far, far)
        inside = jnp.where(late, slot - TILE + far * (TILE // 2), slot)
        result.append((block, chip * TILE + inside))
    return result


def dispatch_kernel(experts, core_ref, token_ref, gain_ref, route_ref, *send_refs):
    tokens = token_ref[...].astype(F32)
    scale = lax.rsqrt(jnp.mean(tokens * tokens, axis=-1, keepdims=True) + NORM_EPS)
    normed = (tokens * scale * gain_ref[...]).astype(BF16)
    places = slots_of(route_ref[...], core_ref[0], experts)
    for block, send_ref in enumerate(send_refs):
        rows = send_ref.shape[0]
        number = lax.broadcasted_iota(jnp.int32, (tokens.shape[0], rows), 1) + block * rows
        chosen = sum((b * rows + p == number).astype(F32) for b, p in places)
        send_ref[...] = mm(chosen.astype(BF16), normed, 0, 0).astype(BF16)


SMEM = pl.BlockSpec(memory_space=pltpu.SMEM)
VMEM = pl.BlockSpec(memory_space=pltpu.VMEM)


def dispatch(core, tokens, gain, routes, experts):
    rows = experts // 2 * TILE
    return pl.pallas_call(
        functools.partial(dispatch_kernel, experts),
        in_specs=[SMEM, VMEM, VMEM, VMEM],
        out_specs=[VMEM] * 4,
        out_shape=[jax.ShapeDtypeStruct((rows, tokens.shape[1]), BF16)] * 4,
        cost_estimate=pl.CostEstimate(
            flops=8 * tokens.size * rows, bytes_accessed=10 * tokens.size, transcendentals=0
        ),
        name="dispatch_rows",
    )(core, tokens, gain.reshape(1, -1), routes)


def combine_kernel(experts, core_ref, weight_ref, route_ref, *refs):
    *back_refs, out_ref = refs
    tokens = weight_ref.shape[0]
    weights = weight_ref[...]
    places = slots_of(route_ref[...], core_ref[0], experts)
    total = jnp.zeros(out_ref.shape, F32)
    for block, ref in enumerate(back_refs):
        rows = ref.shape[0]
        number = lax.broadcasted_iota(jnp.int32, (tokens, rows), 1) + block * rows
        mixed = sum(
            jnp.where(b * rows + p == number, weights[:, k : k + 1], 0.0)
            for k, (b, p) in enumerate(places)
        )
        high = mixed.astype(BF16)
        low = (mixed - high.astype(F32)).astype(BF16)
        total = total + (mm(high, ref[...], 1, 0) + mm(low, ref[...], 1, 0))
    out_ref[...] = total.astype(BF16)


def combine(core, weights, routes, experts, returned):
    tokens = routes.shape[0]
    rows, features = returned[0].shape
    return pl.pallas_call(
        functools.partial(combine_kernel, experts),
        in_specs=[SMEM] + [VMEM] * (2 + len(returned)),
        out_specs=VMEM,
        out_shape=jax.ShapeDtypeStruct((tokens, features), BF16),
        cost_estimate=pl.CostEstimate(
            flops=16 * tokens * rows * features, bytes_accessed=10 * rows * features, transcendentals=0
        ),
        name="combine_rows",
    )(core, weights, routes, *returned)


def clamped_unit(gate_pre, up_pre):
    gate_pre = jnp.minimum(gate_pre, CLAMP_LIMIT)
    up_pre = jnp.clip(up_pre, -CLAMP_LIMIT, CLAMP_LIMIT)
    return (up_pre + 1.0) * gate_pre * jax.nn.sigmoid(SIGMOID_SCALE * gate_pre)


def expert_kernel(pieces, gate_ref, up_ref, down_ref, *refs):
    row_refs, out_refs, rows_ref, total_ref = refs[:pieces], refs[pieces:-2], refs[-2], refs[-1]
    step = pl.program_id(0)

    @pl.when(step == 0)
    def _():
        start = 0
        for ref in row_refs:
            rows_ref[start : start + ref.shape[0], :] = ref[...]
            start += ref.shape[0]
        total_ref[...] = jnp.zeros_like(total_ref)

    rows = rows_ref[...]
    gate_pre = mm(rows, gate_ref[...], 1, 0)
    up_pre = mm(rows, up_ref[...], 1, 0)
    hidden = clamped_unit(gate_pre, up_pre).astype(BF16)
    total_ref[...] += mm(hidden, down_ref[...], 1, 0)

    @pl.when(step == pl.num_programs(0) - 1)
    def _():
        start = 0
        for ref in out_refs:
            ref[...] = total_ref[start : start + ref.shape[0], :].astype(BF16)
            start += ref.shape[0]


def expert_parts(pieces, gate_weight, up_weight, down_weight):
    features, hidden = gate_weight.shape
    width = min(256, hidden)
    rows = sum(p.shape[0] for p in pieces)
    whole = [pl.BlockSpec(p.shape, lambda f: (0, 0)) for p in pieces]
    return pl.pallas_call(
        functools.partial(expert_kernel, len(pieces)),
        grid=(hidden // width,),
        in_specs=[
            pl.BlockSpec((features, width), lambda f: (0, f)),
            pl.BlockSpec((features, width), lambda f: (0, f)),
            pl.BlockSpec((width, features), lambda f: (f, 0)),
            *whole,
        ],
        out_specs=whole,
        out_shape=[jax.ShapeDtypeStruct(p.shape, BF16) for p in pieces],
        scratch_shapes=[pltpu.VMEM((rows, features), BF16), pltpu.VMEM((rows, features), F32)],
        cost_estimate=pl.CostEstimate(
            flops=6 * rows * features * hidden,
            bytes_accessed=6 * features * hidden + 4 * rows * features,
            transcendentals=0,
        ),
        name="expert_parts",
    )(gate_weight, up_weight, down_weight, *pieces)


def turned(x, axis, by):
    size = lax.axis_size(axis)
    return lax.ppermute(x, axis, [(i, (i + by) % size) for i in range(size)])


def gathered_pieces(own):
    half = own.shape[0] // 2
    left = turned(own, "tp", 1)
    right = turned(own, "tp", -1)
    far_low = turned(left[:half], "tp", 1)
    far_high = turned(right[half:], "tp", -1)
    return own, left, right, far_low, far_high


def summed_pieces(parts):
    own, left, right, far_low, far_high = parts
    half = own.shape[0] // 2
    from_right = turned(far_low, "tp", -1)
    from_left = turned(far_high, "tp", 1)
    to_left = jnp.concatenate(
        [(left[:half].astype(F32) + from_right.astype(F32)).astype(BF16), left[half:]], axis=0
    )
    to_right = jnp.concatenate(
        [right[:half], (right[half:].astype(F32) + from_left.astype(F32)).astype(BF16)], axis=0
    )
    back_right = turned(to_left, "tp", -1)
    back_left = turned(to_right, "tp", 1)
    return (own.astype(F32) + back_left.astype(F32) + back_right.astype(F32)).astype(BF16)


def sent_over_chips(rows, chips):
    blocks = rows.reshape(chips, -1, rows.shape[1])
    return lax.all_to_all(blocks, "ep_0", split_axis=0, concat_axis=0, tiled=True).reshape(rows.shape)


def after(value, earlier):
    return lax.optimization_barrier((value, earlier))[0]


def body(
    query,
    forget_gate_logits,
    value,
    forget_lower_margin,
    position_log_decay,
    head_norm_gain,
    mixer_output_weight,
    second_batch_tokens,
    expert_norm_gain,
    routes,
    chosen_expert_weight,
    gate_weight,
    up_weight,
    down_weight,
):
    n_ep = lax.axis_size(EP)
    chips = lax.axis_size("ep_0")
    owners = lax.axis_size("tp")
    core = lax.axis_index("ep_1").astype(jnp.int32).reshape(1)
    place = lax.axis_index(EP).astype(jnp.int32).reshape(1)

    near, far, late_near, late_far = dispatch(
        core, second_batch_tokens, expert_norm_gain, routes, n_ep
    )
    far = turned(far, "ep_1", 1)
    late = late_near + turned(late_far, "ep_1", 1)

    half = mixer_output_weight.shape[0] // 2
    weight_part = lax.dynamic_slice_in_dim(mixer_output_weight, core[0] * half, half, 0)
    weight_mine = lax.all_gather(weight_part, "tp", axis=0, tiled=False)
    weight_other = turned(weight_mine, "ep_1", 1)

    state = mixer_states(
        forget_gate_logits, value, forget_lower_margin, position_log_decay
    )
    gathered = lax.all_gather(state, EP, axis=0, tiled=False)

    sums = []
    arrived = None
    for rows in (near, far, late):
        if arrived is not None:
            rows = after(rows, arrived)
        arrived = sent_over_chips(rows, chips)
        pieces = gathered_pieces(arrived)
        parts = expert_parts(pieces, gate_weight[0], up_weight[0], down_weight[0])
        sums.append(summed_pieces(parts))

    returned = []
    for rows in sums:
        rows = after(rows, returned[-1] if returned else arrived)
        returned.append(sent_over_chips(rows, chips))

    heads = mixer_heads(
        place,
        query,
        forget_gate_logits,
        value,
        forget_lower_margin,
        position_log_decay,
        head_norm_gain,
        gathered,
        owners,
    )
    heads = lax.all_to_all(heads, "tp", split_axis=0, concat_axis=0, tiled=True)
    first_mixer_output = project(core, heads, weight_mine, weight_other)

    back_near, back_far, back_late = returned
    moe_out = combine(
        core,
        chosen_expert_weight,
        routes,
        n_ep,
        (back_near, turned(back_far, "ep_1", 1), back_late, turned(back_late, "ep_1", 1)),
    )
    return (first_mixer_output, moe_out)


def solution(mesh):
    cores = 2
    finer = Mesh(
        mesh.devices.reshape(mesh.shape["grp"], mesh.shape["ep"] // cores, cores, mesh.shape["tp"]),
        ("grp", "ep_0", "ep_1", "tp"),
    )
    placed = (
        P(GRP_EP, "tp"),
        P(GRP_EP, "tp"),
        P(GRP_EP, "tp"),
        P(None, "tp"),
        P("tp", GRP_EP),
        P(),
        P("tp", None),
        P(GRP_EP_TP, None),
        P(),
        P(GRP_EP_TP, None),
        P(GRP_EP_TP, None),
        P(EP, None, "tp"),
        P(EP, None, "tp"),
        P(EP, "tp", None),
    )
    return jax.shard_map(
        body,
        mesh=finer,
        in_specs=placed,
        out_specs=(P(GRP_EP_TP, None), P(GRP_EP_TP, None)),
        check_vma=False,
    )
```

```python
import functools

import jax
import jax.numpy as jnp
from jax import lax
from jax.experimental import pallas as pl
from jax.experimental.pallas import tpu as pltpu
from jax.sharding import Mesh
from jax.sharding import PartitionSpec as P


HEAD_CHANNELS = 128
BLK = 128
STATE_ROWS = HEAD_CHANNELS + 16
EP = ("ep_0", "ep_1")
GRP_EP = ("grp", "ep_0", "ep_1")
GRP_EP_TP = ("grp", "ep_0", "ep_1", "tp")
TILE = 8

NORM_EPS = 1e-06
CLAMP_LIMIT = 7.0
SIGMOID_SCALE = 1.702

F32 = jnp.float32
BF16 = jnp.bfloat16
SMEM = pl.BlockSpec(memory_space=pltpu.SMEM)
VMEM = pl.BlockSpec(memory_space=pltpu.VMEM)


def mm(a, b, lhs_dim, rhs_dim):
    return lax.dot_general(
        a, b, (((lhs_dim,), (rhs_dim,)), ((), ())), preferred_element_type=F32
    )


def pieces_of(x):
    high = x.astype(BF16)
    rest = x - high.astype(F32)
    middle = rest.astype(BF16)
    low = (rest - middle.astype(F32)).astype(BF16)
    return high, middle, low


def summed_along(triangle, x):
    return sum(mm(triangle, piece, 1, 0) for piece in pieces_of(x))


def triangle_of(size, keep):
    rows = lax.broadcasted_iota(jnp.int32, (size, size), 0)
    columns = lax.broadcasted_iota(jnp.int32, (size, size), 1)
    return keep(rows, columns)


def block_gates(logits, margin, decay_row, triangle):
    closing = jnp.exp(margin) * jax.nn.sigmoid(-logits.astype(F32))
    spikes = jnp.transpose(jnp.broadcast_to(decay_row, (BLK, BLK)))
    return closing, summed_along(triangle, jnp.log1p(-closing) + spikes)


def advanced(state, total, closing, cumul, values):
    key_state = (closing * jnp.exp(total - cumul)).astype(BF16)
    return state * jnp.exp(total) + mm(values, key_state, 0, 0)


def rows_of(block):
    return pl.ds(pl.multiple_of(block * BLK, BLK), BLK)


def columns_of(head):
    return slice(head * HEAD_CHANNELS, (head + 1) * HEAD_CHANNELS)


def states_kernel(logits_ref, value_ref, margin_ref, decay_ref, state_ref):
    blocks = logits_ref.shape[0] // BLK
    heads = state_ref.shape[0]
    triangles = (
        triangle_of(BLK, lambda r, c: r >= c).astype(BF16),
        triangle_of(BLK, lambda r, c: r <= c).astype(BF16),
    )
    chains = [(h, d) for h in range(heads) for d in range(2)]

    def step(i, carry):
        after = []
        for (h, d), (state, log) in zip(chains, carry):
            rows = rows_of(i if d == 0 else blocks - 1 - i)
            closing, cumul = block_gates(
                logits_ref[rows, columns_of(h)],
                margin_ref[d : d + 1, columns_of(h)],
                decay_ref[h : h + 1, rows],
                triangles[d],
            )
            total = cumul[BLK - 1 :, :] if d == 0 else cumul[:1, :]
            state = advanced(state, total, closing, cumul, value_ref[rows, columns_of(h)])
            after.append((state, log + total))
        return tuple(after)

    zero = (jnp.zeros((HEAD_CHANNELS, HEAD_CHANNELS), F32), jnp.zeros((1, HEAD_CHANNELS), F32))
    for (h, d), (state, log) in zip(
        chains, lax.fori_loop(0, blocks, step, (zero,) * len(chains))
    ):
        store_state(state_ref, (h, d), state, log)


def mixer_states(logits, value, margin, decay):
    tokens, channels = logits.shape
    heads = channels // HEAD_CHANNELS
    return pl.pallas_call(
        states_kernel,
        in_specs=[VMEM] * 4,
        out_specs=VMEM,
        out_shape=jax.ShapeDtypeStruct((heads, 2, STATE_ROWS, HEAD_CHANNELS), BF16),
        cost_estimate=pl.CostEstimate(
            flops=24 * tokens * channels * BLK, bytes_accessed=5 * tokens * channels, transcendentals=0
        ),
        name="mixer_states",
    )(logits, value, margin, decay)


def decay_of(block):
    tail = block[HEAD_CHANNELS:, :].astype(F32)
    return tail[0:1, :] + tail[1:2, :] + tail[2:3, :]


def store_state(ref, index, state, log):
    places = lax.broadcasted_iota(jnp.int32, (STATE_ROWS - HEAD_CHANNELS, HEAD_CHANNELS), 0)
    tail = jnp.zeros(places.shape, F32)
    for k, piece in enumerate(pieces_of(log)):
        tail = jnp.where(places == k, piece.astype(F32), tail)
    ref[(*index, slice(0, HEAD_CHANNELS), slice(None))] = state.astype(BF16)
    ref[(*index, slice(HEAD_CHANNELS, STATE_ROWS), slice(None))] = tail.astype(BF16)


def merge_kernel(core_ref, own_ref, partner_ref, chip_ref):
    core = core_ref[0]
    for d in range(2):
        own, partner = own_ref[core, d], partner_ref[core, d]
        own_last = (core == 1) if d == 0 else (core == 0)
        first = jnp.where(own_last, partner.astype(F32), own.astype(F32))
        second = jnp.where(own_last, own.astype(F32), partner.astype(F32))
        state = first[:HEAD_CHANNELS] * jnp.exp(decay_of(second)) + second[:HEAD_CHANNELS]
        store_state(chip_ref, (d,), state, decay_of(first) + decay_of(second))


def merged_states(core, own, partner):
    return pl.pallas_call(
        merge_kernel,
        in_specs=[SMEM, VMEM, VMEM],
        out_specs=VMEM,
        out_shape=jax.ShapeDtypeStruct(own.shape[1:], BF16),
        cost_estimate=pl.CostEstimate(flops=8 * own.size, bytes_accessed=5 * own.size, transcendentals=0),
        name="mixer_merge",
    )(core, own, partner)


def entering_kernel(chip_ref, gathered_ref, out_ref):
    chips = gathered_ref.shape[0]
    chip = chip_ref[0]
    for d in range(2):

        def step(i, state):
            j = i if d == 0 else chips - 1 - i
            passed = (j < chip) if d == 0 else (j > chip)
            block = gathered_ref[j, d]
            later = state * jnp.exp(decay_of(block)) + block[:HEAD_CHANNELS, :].astype(F32)
            return jnp.where(passed, later, state)

        zero = jnp.zeros((HEAD_CHANNELS, HEAD_CHANNELS), F32)
        out_ref[d] = lax.fori_loop(0, chips, step, zero).astype(BF16)


def entering_states(chip, gathered):
    return pl.pallas_call(
        entering_kernel,
        in_specs=[SMEM, VMEM],
        out_specs=VMEM,
        out_shape=jax.ShapeDtypeStruct((2, HEAD_CHANNELS, HEAD_CHANNELS), BF16),
        cost_estimate=pl.CostEstimate(
            flops=8 * gathered.size, bytes_accessed=2 * gathered.size, transcendentals=0
        ),
        name="mixer_entering",
    )(chip, gathered)


def heads_kernel(
    place_ref,
    query_ref,
    logits_ref,
    value_ref,
    margin_ref,
    decay_ref,
    gain_ref,
    mine_ref,
    other_ref,
    partner_ref,
    out_ref,
    part_ref,
):
    blocks = logits_ref.shape[0] // BLK
    owners, heads = out_ref.shape[0], out_ref.shape[1]
    per = out_ref.shape[2] // BLK
    core, me = place_ref[0], place_ref[1]
    chains = [(h, d) for h in range(heads) for d in range(2)]

    def entering(h, d):
        state = jnp.where(core == h, mine_ref[d].astype(F32), other_ref[d].astype(F32))
        block = partner_ref[h, d]
        later = state * jnp.exp(decay_of(block)) + block[:HEAD_CHANNELS, :].astype(F32)
        return jnp.where((core == 1) if d == 0 else (core == 0), later, state)

    def part(block, state, h, d):
        rows = rows_of(block)
        keep = triangle_of(BLK, (lambda r, c: r >= c) if d == 0 else (lambda r, c: r <= c))
        values = value_ref[rows, columns_of(h)]
        closing, cumul = block_gates(
            logits_ref[rows, columns_of(h)],
            margin_ref[d : d + 1, columns_of(h)],
            decay_ref[h : h + 1, rows],
            keep.astype(BF16),
        )
        queries = query_ref[rows, columns_of(h)].astype(F32)
        queries = queries * jax.nn.sigmoid(queries) * HEAD_CHANNELS ** (-0.5)
        query_in = (queries * jnp.exp(cumul)).astype(BF16)
        key_in = (closing * jnp.exp(-cumul)).astype(BF16)
        scores = jnp.where(keep, mm(query_in, key_in, 1, 1), 0.0).astype(BF16)
        part_ref[d, rows, columns_of(h)] = mm(scores, values, 1, 0) + mm(
            query_in, state.astype(BF16), 1, 1
        )
        total = cumul[BLK - 1 :, :] if d == 0 else cumul[:1, :]
        return advanced(state, total, closing, cumul, values)

    def step(i, states):
        return tuple(
            part(i if d == 0 else blocks - 1 - i, state, h, d)
            for (h, d), state in zip(chains, states)
        )

    lax.fori_loop(0, blocks, step, tuple(entering(h, d) for h, d in chains))

    def finish(block, _):
        rows = rows_of(block)
        away = lax.rem(block // per - me + owners, owners)
        part_rows = pl.ds(pl.multiple_of((block % per) * BLK, BLK), BLK)
        for h in range(heads):
            mix = part_ref[0, rows, columns_of(h)] + part_ref[1, rows, columns_of(h)]
            scale = lax.rsqrt(jnp.mean(mix * mix, axis=-1, keepdims=True) + NORM_EPS)
            out_ref[away, h, part_rows, :] = (mix * scale * gain_ref[...]).astype(BF16)
        return 0

    lax.fori_loop(0, blocks, finish, 0)


def mixer_heads(place, query, logits, value, margin, decay, gain, mine, other, partner, owners):
    tokens, channels = logits.shape
    heads = channels // HEAD_CHANNELS
    return pl.pallas_call(
        heads_kernel,
        in_specs=[SMEM] + [VMEM] * 9,
        out_specs=VMEM,
        scratch_shapes=[pltpu.VMEM((2, tokens, channels), F32)],
        out_shape=jax.ShapeDtypeStruct((owners, heads, tokens // owners, HEAD_CHANNELS), BF16),
        cost_estimate=pl.CostEstimate(
            flops=48 * tokens * channels * BLK, bytes_accessed=16 * tokens * channels, transcendentals=0
        ),
        name="mixer_heads",
    )(place, query, logits, value, margin, decay, gain.reshape(1, HEAD_CHANNELS), mine, other, partner)


def project_kernel(place_ref, own_ref, left_ref, right_ref, far_ref, mine_ref, other_ref, out_ref):
    core, me = place_ref[0], place_ref[1]
    owners = mine_ref.shape[0]
    width = 256

    def columns(c, _):
        cols = pl.ds(pl.multiple_of(c * width, width), width)
        total = jnp.zeros((out_ref.shape[0], width), F32)
        for ref, by in ((own_ref, 0), (left_ref, owners - 1), (right_ref, 1), (far_ref, 2)):
            source = lax.rem(me + by, owners)
            total += mm(ref[core], mine_ref[source, :, cols], 1, 0)
            total += mm(ref[1 - core], other_ref[source, :, cols], 1, 0)
        out_ref[:, cols] = total.astype(BF16)
        return 0

    lax.fori_loop(0, out_ref.shape[1] // width, columns, 0)


def project(place, heads, mine, other):
    tokens, features = heads[0].shape[1], mine.shape[2]
    return pl.pallas_call(
        project_kernel,
        in_specs=[SMEM] + [VMEM] * 6,
        out_specs=VMEM,
        out_shape=jax.ShapeDtypeStruct((tokens, features), BF16),
        cost_estimate=pl.CostEstimate(
            flops=8 * heads[0].size * features, bytes_accessed=8 * tokens * features, transcendentals=0
        ),
        name="mixer_project",
    )(place, *heads, mine, other)


def slots_of(routes, core, experts):
    top_count, tokens = routes.shape
    number = lax.broadcasted_iota(jnp.int32, (experts, tokens), 0)
    named = [routes[k : k + 1, :] == number for k in range(top_count)]
    counts = sum(n.astype(F32) for n in named).astype(BF16)
    earlier = triangle_of(tokens, lambda r, c: r < c).astype(BF16)
    ranking = mm(counts, earlier, 1, 0)
    result = []
    for k, n in enumerate(named):
        slot = jnp.sum(jnp.where(n, ranking, 0.0), axis=0, keepdims=True).astype(jnp.int32)
        expert = routes[k : k + 1, :]
        chip = expert // 2
        far = jnp.where(expert - 2 * chip == core, 0, 1)
        late = slot >= TILE
        block = jnp.where(late, 2 + far, far)
        inside = jnp.where(late, slot - TILE + far * (TILE // 2), slot)
        result.append((block, chip * TILE + inside))
    return result


def dispatch_kernel(experts, core_ref, token_ref, gain_ref, route_ref, *send_refs):
    tokens = token_ref[...].astype(F32)
    scale = lax.rsqrt(jnp.mean(tokens * tokens, axis=-1, keepdims=True) + NORM_EPS)
    normed = (tokens * scale * gain_ref[...]).astype(BF16)
    places = slots_of(route_ref[...], core_ref[0], experts)
    for block, send_ref in enumerate(send_refs):
        rows = send_ref.shape[0]
        number = lax.broadcasted_iota(jnp.int32, (rows, tokens.shape[0]), 0) + block * rows
        chosen = sum((b * rows + p == number).astype(F32) for b, p in places)
        send_ref[...] = mm(chosen.astype(BF16), normed, 1, 0).astype(BF16)


def dispatch(core, tokens, gain, routes, experts):
    rows = experts // 2 * TILE
    return pl.pallas_call(
        functools.partial(dispatch_kernel, experts),
        in_specs=[SMEM, VMEM, VMEM, VMEM],
        out_specs=[VMEM] * 4,
        out_shape=[jax.ShapeDtypeStruct((rows, tokens.shape[1]), BF16)] * 4,
        cost_estimate=pl.CostEstimate(
            flops=8 * tokens.size * rows, bytes_accessed=10 * tokens.size, transcendentals=0
        ),
        name="dispatch_rows",
    )(core, tokens, gain.reshape(1, -1), routes)


def combine_kernel(experts, first, core_ref, weight_ref, route_ref, *refs):
    back_refs, out_ref = refs[:-1], refs[-1]
    if first:
        base_ref, back_refs = back_refs[0], back_refs[1:]
    weights = weight_ref[...]
    tokens = weights.shape[1]
    places = slots_of(route_ref[...], core_ref[0], experts)
    total = base_ref[...] if first else 0.0
    for block, ref in enumerate(back_refs, first):
        rows = ref.shape[0]
        number = lax.broadcasted_iota(jnp.int32, (rows, tokens), 0) + block * rows
        mixed = sum(
            jnp.where(b * rows + p == number, weights[k : k + 1, :], 0.0)
            for k, (b, p) in enumerate(places)
        )
        high = mixed.astype(BF16)
        low = (mixed - high.astype(F32)).astype(BF16)
        total = total + (mm(high, ref[...], 0, 0) + mm(low, ref[...], 0, 0))
    out_ref[...] = total.astype(out_ref.dtype)


def combine(core, weights, routes, experts, returned, first=0, base=()):
    tokens = routes.shape[1]
    rows, features = returned[0].shape
    return pl.pallas_call(
        functools.partial(combine_kernel, experts, first),
        in_specs=[SMEM] + [VMEM] * (2 + len(base) + len(returned)),
        out_specs=VMEM,
        out_shape=jax.ShapeDtypeStruct((tokens, features), BF16 if first else F32),
        cost_estimate=pl.CostEstimate(
            flops=16 * tokens * rows * features, bytes_accessed=10 * rows * features, transcendentals=0
        ),
        name="combine_rows",
    )(core, weights, routes, *base, *returned)


def clamped_unit(gate_pre, up_pre):
    gate_pre = jnp.minimum(gate_pre, CLAMP_LIMIT)
    up_pre = jnp.clip(up_pre, -CLAMP_LIMIT, CLAMP_LIMIT)
    return (up_pre + 1.0) * gate_pre * jax.nn.sigmoid(SIGMOID_SCALE * gate_pre)


def expert_kernel(pieces, gate_ref, up_ref, down_ref, *refs):
    row_refs, out_refs, rows_ref, total_ref = refs[:pieces], refs[pieces:-2], refs[-2], refs[-1]
    step = pl.program_id(0)

    @pl.when(step == 0)
    def _():
        start = 0
        for ref in row_refs:
            rows_ref[start : start + ref.shape[0], :] = ref[...]
            start += ref.shape[0]
        total_ref[...] = jnp.zeros_like(total_ref)

    rows = rows_ref[...]
    gate_pre = mm(rows, gate_ref[...], 1, 0)
    up_pre = mm(rows, up_ref[...], 1, 0)
    hidden = clamped_unit(gate_pre, up_pre).astype(BF16)
    total_ref[...] += mm(hidden, down_ref[...], 1, 0)

    @pl.when(step == pl.num_programs(0) - 1)
    def _():
        start = 0
        for ref in out_refs:
            ref[...] = total_ref[start : start + ref.shape[0], :].astype(BF16)
            start += ref.shape[0]


def expert_parts(pieces, gate_weight, up_weight, down_weight):
    features, hidden = gate_weight.shape
    width = min(256, hidden)
    rows = sum(p.shape[0] for p in pieces)
    whole = [pl.BlockSpec(p.shape, lambda f: (0, 0)) for p in pieces]
    return pl.pallas_call(
        functools.partial(expert_kernel, len(pieces)),
        grid=(hidden // width,),
        in_specs=[
            pl.BlockSpec((features, width), lambda f: (0, f)),
            pl.BlockSpec((features, width), lambda f: (0, f)),
            pl.BlockSpec((width, features), lambda f: (f, 0)),
            *whole,
        ],
        out_specs=whole,
        out_shape=[jax.ShapeDtypeStruct(p.shape, BF16) for p in pieces],
        scratch_shapes=[pltpu.VMEM((rows, features), BF16), pltpu.VMEM((rows, features), F32)],
        cost_estimate=pl.CostEstimate(
            flops=6 * rows * features * hidden,
            bytes_accessed=6 * features * hidden + 4 * rows * features,
            transcendentals=0,
        ),
        name="expert_parts",
    )(gate_weight, up_weight, down_weight, *pieces)


def turned(x, axis, by):
    size = lax.axis_size(axis)
    return lax.ppermute(x, axis, [(i, (i + by) % size) for i in range(size)])


def gathered_pieces(own):
    half = own.shape[0] // 2
    left = turned(own, "tp", 1)
    right = turned(own, "tp", -1)
    far_low = turned(left[:half], "tp", 1)
    far_high = turned(right[half:], "tp", -1)
    return own, left, right, far_low, far_high


def summed_pieces(parts):
    own, left, right, far_low, far_high = parts
    half = own.shape[0] // 2
    from_right = turned(far_low, "tp", -1)
    from_left = turned(far_high, "tp", 1)
    to_left = jnp.concatenate(
        [(left[:half].astype(F32) + from_right.astype(F32)).astype(BF16), left[half:]], axis=0
    )
    to_right = jnp.concatenate(
        [right[:half], (right[half:].astype(F32) + from_left.astype(F32)).astype(BF16)], axis=0
    )
    back_right = turned(to_left, "tp", -1)
    back_left = turned(to_right, "tp", 1)
    return (own.astype(F32) + back_left.astype(F32) + back_right.astype(F32)).astype(BF16)


def sent_over_chips(rows, chips):
    blocks = rows.reshape(chips, -1, rows.shape[1])
    return lax.all_to_all(blocks, "ep_0", split_axis=0, concat_axis=0, tiled=True).reshape(rows.shape)


def after(value, earlier):
    return lax.optimization_barrier((value, earlier))[0]


def body(
    query,
    forget_gate_logits,
    value,
    forget_lower_margin,
    position_log_decay,
    head_norm_gain,
    mixer_output_weight,
    second_batch_tokens,
    expert_norm_gain,
    routes,
    chosen_expert_weight,
    gate_weight,
    up_weight,
    down_weight,
):
    n_ep = lax.axis_size(EP)
    chips = lax.axis_size("ep_0")
    owners = lax.axis_size("tp")
    core = lax.axis_index("ep_1").astype(jnp.int32).reshape(1)
    chip = lax.axis_index("ep_0").astype(jnp.int32).reshape(1)
    place = jnp.stack([core[0], lax.axis_index("tp").astype(jnp.int32)])

    routes_t, weights_t = jnp.transpose(routes), jnp.transpose(chosen_expert_weight)
    near, far, late_near, late_far = dispatch(
        core, second_batch_tokens, expert_norm_gain, routes_t, n_ep
    )
    far = turned(far, "ep_1", 1)
    late = late_near + turned(late_far, "ep_1", 1)

    state = mixer_states(
        forget_gate_logits, value, forget_lower_margin, position_log_decay
    )
    partner = turned(state, "ep_1", 1)
    chip_state = merged_states(core, state, partner)
    gathered = lax.all_gather(chip_state, "ep_0", axis=0, tiled=False)

    half = mixer_output_weight.shape[0] // 2
    weight_part = lax.dynamic_slice_in_dim(mixer_output_weight, core[0] * half, half, 0)
    weight_part = after(weight_part, chip_state)
    weight_mine = lax.all_gather(weight_part, "tp", axis=0, tiled=False)
    weight_other = turned(weight_mine, "ep_1", 1)

    sums = []
    arrived = None
    for rows in (near, far, late):
        if arrived is not None:
            rows = after(rows, arrived)
        arrived = sent_over_chips(rows, chips)
        pieces = gathered_pieces(arrived)
        parts = expert_parts(pieces, gate_weight[0], up_weight[0], down_weight[0])
        sums.append(summed_pieces(parts))

    returned = []
    for rows in sums:
        rows = after(rows, returned[-1] if returned else arrived)
        returned.append(sent_over_chips(rows, chips))

    entering_mine = entering_states(chip, gathered)
    entering_other = turned(entering_mine, "ep_1", 1)
    heads = mixer_heads(
        place,
        query,
        forget_gate_logits,
        value,
        forget_lower_margin,
        position_log_decay,
        head_norm_gain,
        entering_mine,
        entering_other,
        partner,
        owners,
    )
    heads = (
        heads[0],
        turned(heads[1], "tp", 1),
        turned(heads[owners - 1], "tp", -1),
        turned(heads[2], "tp", 2),
    )
    first_mixer_output = project(place, heads, weight_mine, weight_other)

    back_near, back_far, back_late = returned
    base = combine(core, weights_t, routes_t, n_ep, (back_near, turned(back_far, "ep_1", 1)))
    moe_out = combine(
        core,
        weights_t,
        routes_t,
        n_ep,
        (back_late, turned(back_late, "ep_1", 1)),
        2,
        (base,),
    )
    return (first_mixer_output, moe_out)


def solution(mesh):
    cores = 2
    finer = Mesh(
        mesh.devices.reshape(mesh.shape["grp"], mesh.shape["ep"] // cores, cores, mesh.shape["tp"]),
        ("grp", "ep_0", "ep_1", "tp"),
    )
    placed = (
        P(GRP_EP, "tp"),
        P(GRP_EP, "tp"),
        P(GRP_EP, "tp"),
        P(None, "tp"),
        P("tp", GRP_EP),
        P(),
        P("tp", None),
        P(GRP_EP_TP, None),
        P(),
        P(GRP_EP_TP, None),
        P(GRP_EP_TP, None),
        P(EP, None, "tp"),
        P(EP, None, "tp"),
        P(EP, "tp", None),
    )
    return jax.shard_map(
        body,
        mesh=finer,
        in_specs=placed,
        out_specs=(P(GRP_EP_TP, None), P(GRP_EP_TP, None)),
        check_vma=False,
    )
```

```python
import functools

import jax
import jax.numpy as jnp
from jax import lax
from jax.experimental import pallas as pl
from jax.experimental.pallas import tpu as pltpu
from jax.sharding import Mesh
from jax.sharding import PartitionSpec as P


HEAD_CHANNELS = 128
BLK = 128
STATE_ROWS = HEAD_CHANNELS + 16
EP = ("ep_0", "ep_1")
GRP_EP = ("grp", "ep_0", "ep_1")
GRP_EP_TP = ("grp", "ep_0", "ep_1", "tp")
TILE = 8

NORM_EPS = 1e-06
CLAMP_LIMIT = 7.0
SIGMOID_SCALE = 1.702

F32 = jnp.float32
BF16 = jnp.bfloat16
SMEM = pl.BlockSpec(memory_space=pltpu.SMEM)
VMEM = pl.BlockSpec(memory_space=pltpu.VMEM)


def mm(a, b, lhs_dim, rhs_dim):
    return lax.dot_general(
        a, b, (((lhs_dim,), (rhs_dim,)), ((), ())), preferred_element_type=F32
    )


def pieces_of(x):
    high = x.astype(BF16)
    rest = x - high.astype(F32)
    middle = rest.astype(BF16)
    low = (rest - middle.astype(F32)).astype(BF16)
    return high, middle, low


def summed_along(triangle, x):
    return sum(mm(triangle, piece, 1, 0) for piece in pieces_of(x))


def triangle_of(size, keep):
    rows = lax.broadcasted_iota(jnp.int32, (size, size), 0)
    columns = lax.broadcasted_iota(jnp.int32, (size, size), 1)
    return keep(rows, columns)


def block_gates(logits, margin, decay_row, triangle):
    closing = jnp.exp(margin) * jax.nn.sigmoid(-logits.astype(F32))
    spikes = jnp.transpose(jnp.broadcast_to(decay_row, (BLK, BLK)))
    return closing, summed_along(triangle, jnp.log1p(-closing) + spikes)


def advanced(state, total, closing, cumul, values):
    key_state = (closing * jnp.exp(total - cumul)).astype(BF16)
    return state * jnp.exp(total) + mm(values, key_state, 0, 0)


def rows_of(block):
    return pl.ds(pl.multiple_of(block * BLK, BLK), BLK)


def columns_of(head):
    return slice(head * HEAD_CHANNELS, (head + 1) * HEAD_CHANNELS)


def states_kernel(logits_ref, value_ref, margin_ref, decay_ref, state_ref):
    blocks = logits_ref.shape[0] // BLK
    heads = state_ref.shape[0]
    triangles = (
        triangle_of(BLK, lambda r, c: r >= c).astype(BF16),
        triangle_of(BLK, lambda r, c: r <= c).astype(BF16),
    )
    chains = [(h, d) for h in range(heads) for d in range(2)]

    def step(i, carry):
        after = []
        for (h, d), (state, log) in zip(chains, carry):
            rows = rows_of(i if d == 0 else blocks - 1 - i)
            closing, cumul = block_gates(
                logits_ref[rows, columns_of(h)],
                margin_ref[d : d + 1, columns_of(h)],
                decay_ref[h : h + 1, rows],
                triangles[d],
            )
            total = cumul[BLK - 1 :, :] if d == 0 else cumul[:1, :]
            state = advanced(state, total, closing, cumul, value_ref[rows, columns_of(h)])
            after.append((state, log + total))
        return tuple(after)

    zero = (jnp.zeros((HEAD_CHANNELS, HEAD_CHANNELS), F32), jnp.zeros((1, HEAD_CHANNELS), F32))
    for (h, d), (state, log) in zip(
        chains, lax.fori_loop(0, blocks, step, (zero,) * len(chains))
    ):
        store_state(state_ref, (h, d), state, log)


def mixer_states(logits, value, margin, decay):
    tokens, channels = logits.shape
    heads = channels // HEAD_CHANNELS
    return pl.pallas_call(
        states_kernel,
        in_specs=[VMEM] * 4,
        out_specs=VMEM,
        out_shape=jax.ShapeDtypeStruct((heads, 2, STATE_ROWS, HEAD_CHANNELS), BF16),
        cost_estimate=pl.CostEstimate(
            flops=24 * tokens * channels * BLK, bytes_accessed=5 * tokens * channels, transcendentals=0
        ),
        name="mixer_states",
    )(logits, value, margin, decay)


def decay_of(block):
    tail = block[HEAD_CHANNELS:, :].astype(F32)
    return tail[0:1, :] + tail[1:2, :] + tail[2:3, :]


def store_state(ref, index, state, log):
    places = lax.broadcasted_iota(jnp.int32, (STATE_ROWS - HEAD_CHANNELS, HEAD_CHANNELS), 0)
    tail = jnp.zeros(places.shape, F32)
    for k, piece in enumerate(pieces_of(log)):
        tail = jnp.where(places == k, piece.astype(F32), tail)
    ref[(*index, slice(0, HEAD_CHANNELS), slice(None))] = state.astype(BF16)
    ref[(*index, slice(HEAD_CHANNELS, STATE_ROWS), slice(None))] = tail.astype(BF16)


def merge_kernel(core_ref, own_ref, partner_ref, chip_ref):
    core = core_ref[0]
    for d in range(2):
        own, partner = own_ref[core, d], partner_ref[core, d]
        own_last = (core == 1) if d == 0 else (core == 0)
        first = jnp.where(own_last, partner.astype(F32), own.astype(F32))
        second = jnp.where(own_last, own.astype(F32), partner.astype(F32))
        state = first[:HEAD_CHANNELS] * jnp.exp(decay_of(second)) + second[:HEAD_CHANNELS]
        store_state(chip_ref, (d,), state, decay_of(first) + decay_of(second))


def merged_states(core, own, partner):
    return pl.pallas_call(
        merge_kernel,
        in_specs=[SMEM, VMEM, VMEM],
        out_specs=VMEM,
        out_shape=jax.ShapeDtypeStruct(own.shape[1:], BF16),
        cost_estimate=pl.CostEstimate(flops=8 * own.size, bytes_accessed=5 * own.size, transcendentals=0),
        name="mixer_merge",
    )(core, own, partner)


def entering_kernel(chip_ref, gathered_ref, out_ref):
    chips = gathered_ref.shape[0]
    chip = chip_ref[0]
    for d in range(2):

        def step(i, state):
            j = i if d == 0 else chips - 1 - i
            passed = (j < chip) if d == 0 else (j > chip)
            block = gathered_ref[j, d]
            later = state * jnp.exp(decay_of(block)) + block[:HEAD_CHANNELS, :].astype(F32)
            return jnp.where(passed, later, state)

        zero = jnp.zeros((HEAD_CHANNELS, HEAD_CHANNELS), F32)
        out_ref[d] = lax.fori_loop(0, chips, step, zero).astype(BF16)


def entering_states(chip, gathered):
    return pl.pallas_call(
        entering_kernel,
        in_specs=[SMEM, VMEM],
        out_specs=VMEM,
        out_shape=jax.ShapeDtypeStruct((2, HEAD_CHANNELS, HEAD_CHANNELS), BF16),
        cost_estimate=pl.CostEstimate(
            flops=8 * gathered.size, bytes_accessed=2 * gathered.size, transcendentals=0
        ),
        name="mixer_entering",
    )(chip, gathered)


def heads_kernel(
    place_ref,
    query_ref,
    logits_ref,
    value_ref,
    margin_ref,
    decay_ref,
    gain_ref,
    mine_ref,
    other_ref,
    partner_ref,
    out_ref,
    part_ref,
):
    blocks = logits_ref.shape[0] // BLK
    owners, heads = out_ref.shape[0], out_ref.shape[1]
    per = out_ref.shape[2] // BLK
    core, me = place_ref[0], place_ref[1]
    chains = [(h, d) for h in range(heads) for d in range(2)]

    def entering(h, d):
        state = jnp.where(core == h, mine_ref[d].astype(F32), other_ref[d].astype(F32))
        block = partner_ref[h, d]
        later = state * jnp.exp(decay_of(block)) + block[:HEAD_CHANNELS, :].astype(F32)
        return jnp.where((core == 1) if d == 0 else (core == 0), later, state)

    def part(block, state, h, d):
        rows = rows_of(block)
        keep = triangle_of(BLK, (lambda r, c: r >= c) if d == 0 else (lambda r, c: r <= c))
        values = value_ref[rows, columns_of(h)]
        closing, cumul = block_gates(
            logits_ref[rows, columns_of(h)],
            margin_ref[d : d + 1, columns_of(h)],
            decay_ref[h : h + 1, rows],
            keep.astype(BF16),
        )
        queries = query_ref[rows, columns_of(h)].astype(F32)
        queries = queries * jax.nn.sigmoid(queries) * HEAD_CHANNELS ** (-0.5)
        query_in = (queries * jnp.exp(cumul)).astype(BF16)
        key_in = (closing * jnp.exp(-cumul)).astype(BF16)
        scores = jnp.where(keep, mm(query_in, key_in, 1, 1), 0.0).astype(BF16)
        part_ref[d, rows, columns_of(h)] = mm(scores, values, 1, 0) + mm(
            query_in, state.astype(BF16), 1, 1
        )
        total = cumul[BLK - 1 :, :] if d == 0 else cumul[:1, :]
        return advanced(state, total, closing, cumul, values)

    def step(i, states):
        return tuple(
            part(i if d == 0 else blocks - 1 - i, state, h, d)
            for (h, d), state in zip(chains, states)
        )

    lax.fori_loop(0, blocks, step, tuple(entering(h, d) for h, d in chains))

    def finish(block, _):
        rows = rows_of(block)
        away = lax.rem(block // per - me + owners, owners)
        part_rows = pl.ds(pl.multiple_of((block % per) * BLK, BLK), BLK)
        for h in range(heads):
            mix = part_ref[0, rows, columns_of(h)] + part_ref[1, rows, columns_of(h)]
            scale = lax.rsqrt(jnp.mean(mix * mix, axis=-1, keepdims=True) + NORM_EPS)
            out_ref[away, h, part_rows, :] = (mix * scale * gain_ref[...]).astype(BF16)
        return 0

    lax.fori_loop(0, blocks, finish, 0)


def mixer_heads(place, query, logits, value, margin, decay, gain, mine, other, partner, owners):
    tokens, channels = logits.shape
    heads = channels // HEAD_CHANNELS
    return pl.pallas_call(
        heads_kernel,
        in_specs=[SMEM] + [VMEM] * 9,
        out_specs=VMEM,
        scratch_shapes=[pltpu.VMEM((2, tokens, channels), F32)],
        out_shape=jax.ShapeDtypeStruct((owners, heads, tokens // owners, HEAD_CHANNELS), BF16),
        cost_estimate=pl.CostEstimate(
            flops=48 * tokens * channels * BLK, bytes_accessed=16 * tokens * channels, transcendentals=0
        ),
        name="mixer_heads",
    )(place, query, logits, value, margin, decay, gain.reshape(1, HEAD_CHANNELS), mine, other, partner)


def project_kernel(place_ref, own_ref, left_ref, right_ref, far_ref, mine_ref, other_ref, out_ref):
    core, me = place_ref[0], place_ref[1]
    owners = mine_ref.shape[0]
    width = 256

    def columns(c, _):
        cols = pl.ds(pl.multiple_of(c * width, width), width)
        total = jnp.zeros((out_ref.shape[0], width), F32)
        for ref, by in ((own_ref, 0), (left_ref, owners - 1), (right_ref, 1), (far_ref, 2)):
            source = lax.rem(me + by, owners)
            total += mm(ref[core], mine_ref[source, :, cols], 1, 0)
            total += mm(ref[1 - core], other_ref[source, :, cols], 1, 0)
        out_ref[:, cols] = total.astype(BF16)
        return 0

    lax.fori_loop(0, out_ref.shape[1] // width, columns, 0)


def project(place, heads, mine, other):
    tokens, features = heads[0].shape[1], mine.shape[2]
    return pl.pallas_call(
        project_kernel,
        in_specs=[SMEM] + [VMEM] * 6,
        out_specs=VMEM,
        out_shape=jax.ShapeDtypeStruct((tokens, features), BF16),
        cost_estimate=pl.CostEstimate(
            flops=8 * heads[0].size * features, bytes_accessed=8 * tokens * features, transcendentals=0
        ),
        name="mixer_project",
    )(place, *heads, mine, other)


def slots_of(routes, core, experts):
    top_count, tokens = routes.shape
    number = lax.broadcasted_iota(jnp.int32, (experts, tokens), 0)
    named = [routes[k : k + 1, :] == number for k in range(top_count)]
    counts = sum(n.astype(F32) for n in named).astype(BF16)
    earlier = triangle_of(tokens, lambda r, c: r < c).astype(BF16)
    ranking = mm(counts, earlier, 1, 0)
    result = []
    for k, n in enumerate(named):
        slot = jnp.sum(jnp.where(n, ranking, 0.0), axis=0, keepdims=True).astype(jnp.int32)
        expert = routes[k : k + 1, :]
        chip = expert // 2
        far = jnp.where(expert - 2 * chip == core, 0, 1)
        late = slot >= TILE
        block = jnp.where(late, 2 + far, far)
        inside = jnp.where(late, slot - TILE + far * (TILE // 2), slot)
        result.append((block, chip * TILE + inside))
    return result


def dispatch_kernel(experts, core_ref, token_ref, gain_ref, route_ref, *send_refs):
    tokens = token_ref[...].astype(F32)
    scale = lax.rsqrt(jnp.mean(tokens * tokens, axis=-1, keepdims=True) + NORM_EPS)
    normed = (tokens * scale * gain_ref[...]).astype(BF16)
    places = slots_of(route_ref[...], core_ref[0], experts)
    for block, send_ref in enumerate(send_refs):
        rows = send_ref.shape[0]
        number = lax.broadcasted_iota(jnp.int32, (rows, tokens.shape[0]), 0) + block * rows
        chosen = sum((b * rows + p == number).astype(F32) for b, p in places)
        send_ref[...] = mm(chosen.astype(BF16), normed, 1, 0).astype(BF16)


def dispatch(core, tokens, gain, routes, experts):
    rows = experts // 2 * TILE
    return pl.pallas_call(
        functools.partial(dispatch_kernel, experts),
        in_specs=[SMEM, VMEM, VMEM, VMEM],
        out_specs=[VMEM] * 4,
        out_shape=[jax.ShapeDtypeStruct((rows, tokens.shape[1]), BF16)] * 4,
        cost_estimate=pl.CostEstimate(
            flops=8 * tokens.size * rows, bytes_accessed=10 * tokens.size, transcendentals=0
        ),
        name="dispatch_rows",
    )(core, tokens, gain.reshape(1, -1), routes)


def combine_kernel(experts, first, core_ref, weight_ref, route_ref, *refs):
    back_refs, out_ref = refs[:-1], refs[-1]
    if first:
        base_ref, back_refs = back_refs[0], back_refs[1:]
    weights = weight_ref[...]
    tokens = weights.shape[1]
    places = slots_of(route_ref[...], core_ref[0], experts)
    total = base_ref[...] if first else 0.0
    for block, ref in enumerate(back_refs, first):
        rows = ref.shape[0]
        number = lax.broadcasted_iota(jnp.int32, (rows, tokens), 0) + block * rows
        mixed = sum(
            jnp.where(b * rows + p == number, weights[k : k + 1, :], 0.0)
            for k, (b, p) in enumerate(places)
        )
        high = mixed.astype(BF16)
        low = (mixed - high.astype(F32)).astype(BF16)
        total = total + (mm(high, ref[...], 0, 0) + mm(low, ref[...], 0, 0))
    out_ref[...] = total.astype(out_ref.dtype)


def combine(core, weights, routes, experts, returned, first=0, base=()):
    tokens = routes.shape[1]
    rows, features = returned[0].shape
    return pl.pallas_call(
        functools.partial(combine_kernel, experts, first),
        in_specs=[SMEM] + [VMEM] * (2 + len(base) + len(returned)),
        out_specs=VMEM,
        out_shape=jax.ShapeDtypeStruct((tokens, features), BF16 if first else F32),
        cost_estimate=pl.CostEstimate(
            flops=16 * tokens * rows * features, bytes_accessed=10 * rows * features, transcendentals=0
        ),
        name="combine_rows",
    )(core, weights, routes, *base, *returned)


def clamped_unit(gate_pre, up_pre):
    gate_pre = jnp.minimum(gate_pre, CLAMP_LIMIT)
    up_pre = jnp.clip(up_pre, -CLAMP_LIMIT, CLAMP_LIMIT)
    return (up_pre + 1.0) * gate_pre * jax.nn.sigmoid(SIGMOID_SCALE * gate_pre)


def expert_kernel(pieces, me_ref, gate_ref, up_ref, down_ref, *refs):
    row_refs, out_refs, rows_ref, total_ref = refs[:pieces], refs[pieces:-2], refs[-2], refs[-1]
    step = pl.program_id(0)

    @pl.when(step == 0)
    def _():
        start = 0
        for ref in row_refs:
            rows_ref[start : start + ref.shape[0], :] = ref[...]
            start += ref.shape[0]
        total_ref[...] = jnp.zeros_like(total_ref)

    rows = rows_ref[...]
    gate_pre = mm(rows, gate_ref[...], 1, 0)
    up_pre = mm(rows, up_ref[...], 1, 0)
    hidden = clamped_unit(gate_pre, up_pre).astype(BF16)
    total_ref[...] += mm(hidden, down_ref[...], 1, 0)

    @pl.when(step == pl.num_programs(0) - 1)
    def _():
        if len(out_refs) > 1:
            start = 0
            for ref in out_refs:
                ref[...] = total_ref[start : start + ref.shape[0], :].astype(BF16)
                start += ref.shape[0]
        else:
            (ref,) = out_refs
            owners, per = ref.shape[0], ref.shape[1]
            for k, by in enumerate((0, owners - 1, 1, 2)):
                owner = lax.rem(me_ref[0] + by, owners)
                ref[owner] = total_ref[k * per : (k + 1) * per, :].astype(BF16)


def expert_parts(me, pieces, gate_weight, up_weight, down_weight, owners=None):
    features, hidden = gate_weight.shape
    width = min(256, hidden)
    rows = sum(p.shape[0] for p in pieces)
    whole = [pl.BlockSpec(p.shape, lambda f: (0, 0)) for p in pieces]
    out_specs, out_shape = whole, [jax.ShapeDtypeStruct(p.shape, BF16) for p in pieces]
    if owners:
        by_owner = (owners, rows // owners, features)
        out_specs = [pl.BlockSpec(by_owner, lambda f: (0, 0, 0))]
        out_shape = [jax.ShapeDtypeStruct(by_owner, BF16)]
    return pl.pallas_call(
        functools.partial(expert_kernel, len(pieces)),
        grid=(hidden // width,),
        in_specs=[
            SMEM,
            pl.BlockSpec((features, width), lambda f: (0, f)),
            pl.BlockSpec((features, width), lambda f: (0, f)),
            pl.BlockSpec((width, features), lambda f: (f, 0)),
            *whole,
        ],
        out_specs=out_specs,
        out_shape=out_shape,
        scratch_shapes=[pltpu.VMEM((rows, features), BF16), pltpu.VMEM((rows, features), F32)],
        cost_estimate=pl.CostEstimate(
            flops=6 * rows * features * hidden,
            bytes_accessed=6 * features * hidden + 4 * rows * features,
            transcendentals=0,
        ),
        name="expert_parts",
    )(me, gate_weight, up_weight, down_weight, *pieces)


def turned(x, axis, by):
    size = lax.axis_size(axis)
    return lax.ppermute(x, axis, [(i, (i + by) % size) for i in range(size)])


def gathered_pieces(own):
    half = own.shape[0] // 2
    left = turned(own, "tp", 1)
    right = turned(own, "tp", -1)
    far_low = turned(left[:half], "tp", 1)
    far_high = turned(right[half:], "tp", -1)
    return own, left, right, far_low, far_high


def summed_pieces(parts):
    own, left, right, far_low, far_high = parts
    half = own.shape[0] // 2
    from_right = turned(far_low, "tp", -1)
    from_left = turned(far_high, "tp", 1)
    low = (left[:half].astype(F32) + from_right.astype(F32)).astype(BF16)
    high = (right[half:].astype(F32) + from_left.astype(F32)).astype(BF16)
    to_left = jnp.concatenate([low, left[half:]], axis=0)
    to_right = jnp.concatenate([right[:half], high], axis=0)
    back_right = turned(to_left, "tp", -1)
    back_left = turned(to_right, "tp", 1)
    return (own.astype(F32) + back_left.astype(F32) + back_right.astype(F32)).astype(BF16)


def sent_over_chips(rows, chips):
    blocks = rows.reshape(chips, -1, rows.shape[1])
    return lax.all_to_all(blocks, "ep_0", split_axis=0, concat_axis=0, tiled=True).reshape(rows.shape)


def after(value, earlier):
    return lax.optimization_barrier((value, earlier))[0]


def body(
    query,
    forget_gate_logits,
    value,
    forget_lower_margin,
    position_log_decay,
    head_norm_gain,
    mixer_output_weight,
    second_batch_tokens,
    expert_norm_gain,
    routes,
    chosen_expert_weight,
    gate_weight,
    up_weight,
    down_weight,
):
    n_ep = lax.axis_size(EP)
    chips = lax.axis_size("ep_0")
    owners = lax.axis_size("tp")
    core = lax.axis_index("ep_1").astype(jnp.int32).reshape(1)
    chip = lax.axis_index("ep_0").astype(jnp.int32).reshape(1)
    me = lax.axis_index("tp").astype(jnp.int32).reshape(1)
    place = jnp.stack([core[0], lax.axis_index("tp").astype(jnp.int32)])

    half = mixer_output_weight.shape[0] // 2
    weight_part = lax.dynamic_slice_in_dim(mixer_output_weight, core[0] * half, half, 0)
    weight_mine = lax.all_gather(weight_part, "tp", axis=0, tiled=False)
    weight_other = turned(weight_mine, "ep_1", 1)

    routes_t, weights_t = jnp.transpose(routes), jnp.transpose(chosen_expert_weight)
    near, far, late_near, late_far = dispatch(
        core, after(second_batch_tokens, weight_part), expert_norm_gain, routes_t, n_ep
    )
    far = turned(far, "ep_1", 1)
    late = late_near + turned(late_far, "ep_1", 1)

    state = mixer_states(
        forget_gate_logits, value, forget_lower_margin, position_log_decay
    )
    partner = turned(state, "ep_1", 1)
    chip_state = merged_states(core, state, partner)
    gathered = lax.all_gather(chip_state, "ep_0", axis=0, tiled=False)

    sums = []
    arrived = None
    for c, rows in enumerate((near, far, late)):
        if arrived is not None:
            rows = after(rows, (arrived, late))
        arrived = sent_over_chips(rows, chips)
        pieces = gathered_pieces(arrived)
        if not c:
            pieces = after(pieces, weight_mine)
        parts = expert_parts(
            me,
            pieces,
            gate_weight[0],
            up_weight[0],
            down_weight[0],
            owners if c else None,
        )
        if c:
            parts = parts[0].reshape(owners * rows.shape[0], -1)
            sums.append(lax.psum_scatter(parts, "tp", scatter_dimension=0, tiled=True))
        else:
            sums.append(summed_pieces(parts))

    returned = []
    for rows in sums:
        rows = after(rows, returned[-1] if returned else arrived)
        returned.append(sent_over_chips(rows, chips))

    entering_mine = entering_states(chip, gathered)
    entering_other = turned(entering_mine, "ep_1", 1)
    heads = mixer_heads(
        place,
        query,
        forget_gate_logits,
        value,
        forget_lower_margin,
        position_log_decay,
        head_norm_gain,
        entering_mine,
        entering_other,
        partner,
        owners,
    )
    heads = (
        heads[0],
        turned(heads[1], "tp", 1),
        turned(heads[owners - 1], "tp", -1),
        turned(heads[2], "tp", 2),
    )
    first_mixer_output = project(place, heads, weight_mine, weight_other)

    back_near, back_far, back_late = returned
    base = combine(core, weights_t, routes_t, n_ep, (back_near, turned(back_far, "ep_1", 1)))
    moe_out = combine(
        core,
        weights_t,
        routes_t,
        n_ep,
        (back_late, turned(back_late, "ep_1", 1)),
        2,
        (base,),
    )
    return (first_mixer_output, moe_out)


def solution(mesh):
    cores = 2
    finer = Mesh(
        mesh.devices.reshape(mesh.shape["grp"], mesh.shape["ep"] // cores, cores, mesh.shape["tp"]),
        ("grp", "ep_0", "ep_1", "tp"),
    )
    placed = (
        P(GRP_EP, "tp"),
        P(GRP_EP, "tp"),
        P(GRP_EP, "tp"),
        P(None, "tp"),
        P("tp", GRP_EP),
        P(),
        P("tp", None),
        P(GRP_EP_TP, None),
        P(),
        P(GRP_EP_TP, None),
        P(GRP_EP_TP, None),
        P(EP, None, "tp"),
        P(EP, None, "tp"),
        P(EP, "tp", None),
    )
    return jax.shard_map(
        body,
        mesh=finer,
        in_specs=placed,
        out_specs=(P(GRP_EP_TP, None), P(GRP_EP_TP, None)),
        check_vma=False,
    )
```

```python
import functools

import jax
import jax.numpy as jnp
from jax import lax
from jax.experimental import pallas as pl
from jax.experimental.pallas import tpu as pltpu
from jax.sharding import Mesh
from jax.sharding import PartitionSpec as P


HEAD_CHANNELS = 128
BLK = 128
STATE_ROWS = HEAD_CHANNELS + 16
EP = ("ep_0", "ep_1")
GRP_EP = ("grp", "ep_0", "ep_1")
GRP_EP_TP = ("grp", "ep_0", "ep_1", "tp")
TILE = 8

NORM_EPS = 1e-06
CLAMP_LIMIT = 7.0
SIGMOID_SCALE = 1.702

F32 = jnp.float32
BF16 = jnp.bfloat16
SMEM = pl.BlockSpec(memory_space=pltpu.SMEM)
VMEM = pl.BlockSpec(memory_space=pltpu.VMEM)


def mm(a, b, lhs_dim, rhs_dim):
    return lax.dot_general(
        a, b, (((lhs_dim,), (rhs_dim,)), ((), ())), preferred_element_type=F32
    )


def pieces_of(x):
    high = x.astype(BF16)
    rest = x - high.astype(F32)
    middle = rest.astype(BF16)
    low = (rest - middle.astype(F32)).astype(BF16)
    return high, middle, low


def summed_along(triangle, x):
    return sum(mm(triangle, piece, 1, 0) for piece in pieces_of(x))


def triangle_of(size, keep):
    rows = lax.broadcasted_iota(jnp.int32, (size, size), 0)
    columns = lax.broadcasted_iota(jnp.int32, (size, size), 1)
    return keep(rows, columns)


def block_gates(logits, margin, decay_row, triangle):
    closing = jnp.exp(margin) * jax.nn.sigmoid(-logits.astype(F32))
    spikes = jnp.transpose(jnp.broadcast_to(decay_row, (BLK, BLK)))
    return closing, summed_along(triangle, jnp.log1p(-closing) + spikes)


def advanced(state, total, closing, cumul, values):
    key_state = (closing * jnp.exp(total - cumul)).astype(BF16)
    return state * jnp.exp(total) + mm(values, key_state, 0, 0)


def rows_of(block):
    return pl.ds(pl.multiple_of(block * BLK, BLK), BLK)


def columns_of(head):
    return slice(head * HEAD_CHANNELS, (head + 1) * HEAD_CHANNELS)


def states_kernel(logits_ref, value_ref, margin_ref, decay_ref, state_ref):
    blocks = logits_ref.shape[0] // BLK
    heads = state_ref.shape[0]
    triangles = (
        triangle_of(BLK, lambda r, c: r >= c).astype(BF16),
        triangle_of(BLK, lambda r, c: r <= c).astype(BF16),
    )
    chains = [(h, d) for h in range(heads) for d in range(2)]

    def step(i, carry):
        after = []
        for (h, d), (state, log) in zip(chains, carry):
            rows = rows_of(i if d == 0 else blocks - 1 - i)
            closing, cumul = block_gates(
                logits_ref[rows, columns_of(h)],
                margin_ref[d : d + 1, columns_of(h)],
                decay_ref[h : h + 1, rows],
                triangles[d],
            )
            total = cumul[BLK - 1 :, :] if d == 0 else cumul[:1, :]
            state = advanced(state, total, closing, cumul, value_ref[rows, columns_of(h)])
            after.append((state, log + total))
        return tuple(after)

    zero = (jnp.zeros((HEAD_CHANNELS, HEAD_CHANNELS), F32), jnp.zeros((1, HEAD_CHANNELS), F32))
    for (h, d), (state, log) in zip(
        chains, lax.fori_loop(0, blocks, step, (zero,) * len(chains))
    ):
        store_state(state_ref, (h, d), state, log)


def mixer_states(logits, value, margin, decay):
    tokens, channels = logits.shape
    heads = channels // HEAD_CHANNELS
    return pl.pallas_call(
        states_kernel,
        in_specs=[VMEM] * 4,
        out_specs=VMEM,
        out_shape=jax.ShapeDtypeStruct((heads, 2, STATE_ROWS, HEAD_CHANNELS), BF16),
        cost_estimate=pl.CostEstimate(
            flops=24 * tokens * channels * BLK, bytes_accessed=5 * tokens * channels, transcendentals=0
        ),
        name="mixer_states",
    )(logits, value, margin, decay)


def decay_of(block):
    tail = block[HEAD_CHANNELS:, :].astype(F32)
    return tail[0:1, :] + tail[1:2, :] + tail[2:3, :]


def store_state(ref, index, state, log):
    places = lax.broadcasted_iota(jnp.int32, (STATE_ROWS - HEAD_CHANNELS, HEAD_CHANNELS), 0)
    tail = jnp.zeros(places.shape, F32)
    for k, piece in enumerate(pieces_of(log)):
        tail = jnp.where(places == k, piece.astype(F32), tail)
    ref[(*index, slice(0, HEAD_CHANNELS), slice(None))] = state.astype(BF16)
    ref[(*index, slice(HEAD_CHANNELS, STATE_ROWS), slice(None))] = tail.astype(BF16)


def merge_kernel(core_ref, own_ref, partner_ref, chip_ref):
    core = core_ref[0]
    for d in range(2):
        own, partner = own_ref[core, d], partner_ref[core, d]
        own_last = (core == 1) if d == 0 else (core == 0)
        first = jnp.where(own_last, partner.astype(F32), own.astype(F32))
        second = jnp.where(own_last, own.astype(F32), partner.astype(F32))
        state = first[:HEAD_CHANNELS] * jnp.exp(decay_of(second)) + second[:HEAD_CHANNELS]
        store_state(chip_ref, (d,), state, decay_of(first) + decay_of(second))


def merged_states(core, own, partner):
    return pl.pallas_call(
        merge_kernel,
        in_specs=[SMEM, VMEM, VMEM],
        out_specs=VMEM,
        out_shape=jax.ShapeDtypeStruct(own.shape[1:], BF16),
        cost_estimate=pl.CostEstimate(flops=8 * own.size, bytes_accessed=5 * own.size, transcendentals=0),
        name="mixer_merge",
    )(core, own, partner)


def entering_kernel(chip_ref, gathered_ref, out_ref):
    chips = gathered_ref.shape[0]
    chip = chip_ref[0]
    for d in range(2):

        def step(i, state):
            j = i if d == 0 else chips - 1 - i
            passed = (j < chip) if d == 0 else (j > chip)
            block = gathered_ref[j, d]
            later = state * jnp.exp(decay_of(block)) + block[:HEAD_CHANNELS, :].astype(F32)
            return jnp.where(passed, later, state)

        zero = jnp.zeros((HEAD_CHANNELS, HEAD_CHANNELS), F32)
        out_ref[d] = lax.fori_loop(0, chips, step, zero).astype(BF16)


def entering_states(chip, gathered):
    return pl.pallas_call(
        entering_kernel,
        in_specs=[SMEM, VMEM],
        out_specs=VMEM,
        out_shape=jax.ShapeDtypeStruct((2, HEAD_CHANNELS, HEAD_CHANNELS), BF16),
        cost_estimate=pl.CostEstimate(
            flops=8 * gathered.size, bytes_accessed=2 * gathered.size, transcendentals=0
        ),
        name="mixer_entering",
    )(chip, gathered)


def heads_kernel(
    place_ref,
    query_ref,
    logits_ref,
    value_ref,
    margin_ref,
    decay_ref,
    gain_ref,
    mine_ref,
    other_ref,
    partner_ref,
    out_ref,
    part_ref,
):
    blocks = logits_ref.shape[0] // BLK
    owners, heads = out_ref.shape[0], out_ref.shape[1]
    per = out_ref.shape[2] // BLK
    core, me = place_ref[0], place_ref[1]
    chains = [(h, d) for h in range(heads) for d in range(2)]

    def entering(h, d):
        state = jnp.where(core == h, mine_ref[d].astype(F32), other_ref[d].astype(F32))
        block = partner_ref[h, d]
        later = state * jnp.exp(decay_of(block)) + block[:HEAD_CHANNELS, :].astype(F32)
        return jnp.where((core == 1) if d == 0 else (core == 0), later, state)

    def part(block, state, h, d):
        rows = rows_of(block)
        keep = triangle_of(BLK, (lambda r, c: r >= c) if d == 0 else (lambda r, c: r <= c))
        values = value_ref[rows, columns_of(h)]
        closing, cumul = block_gates(
            logits_ref[rows, columns_of(h)],
            margin_ref[d : d + 1, columns_of(h)],
            decay_ref[h : h + 1, rows],
            keep.astype(BF16),
        )
        queries = query_ref[rows, columns_of(h)].astype(F32)
        queries = queries * jax.nn.sigmoid(queries) * HEAD_CHANNELS ** (-0.5)
        query_in = (queries * jnp.exp(cumul)).astype(BF16)
        key_in = (closing * jnp.exp(-cumul)).astype(BF16)
        scores = jnp.where(keep, mm(query_in, key_in, 1, 1), 0.0).astype(BF16)
        part_ref[d, rows, columns_of(h)] = mm(scores, values, 1, 0) + mm(
            query_in, state.astype(BF16), 1, 1
        )
        total = cumul[BLK - 1 :, :] if d == 0 else cumul[:1, :]
        return advanced(state, total, closing, cumul, values)

    def step(i, states):
        return tuple(
            part(i if d == 0 else blocks - 1 - i, state, h, d)
            for (h, d), state in zip(chains, states)
        )

    lax.fori_loop(0, blocks, step, tuple(entering(h, d) for h, d in chains))

    def finish(block, _):
        rows = rows_of(block)
        away = lax.rem(block // per - me + owners, owners)
        part_rows = pl.ds(pl.multiple_of((block % per) * BLK, BLK), BLK)
        for h in range(heads):
            mix = part_ref[0, rows, columns_of(h)] + part_ref[1, rows, columns_of(h)]
            scale = lax.rsqrt(jnp.mean(mix * mix, axis=-1, keepdims=True) + NORM_EPS)
            out_ref[away, h, part_rows, :] = (mix * scale * gain_ref[...]).astype(BF16)
        return 0

    lax.fori_loop(0, blocks, finish, 0)


def mixer_heads(place, query, logits, value, margin, decay, gain, mine, other, partner, owners):
    tokens, channels = logits.shape
    heads = channels // HEAD_CHANNELS
    return pl.pallas_call(
        heads_kernel,
        in_specs=[SMEM] + [VMEM] * 9,
        out_specs=VMEM,
        scratch_shapes=[pltpu.VMEM((2, tokens, channels), F32)],
        out_shape=jax.ShapeDtypeStruct((owners, heads, tokens // owners, HEAD_CHANNELS), BF16),
        cost_estimate=pl.CostEstimate(
            flops=48 * tokens * channels * BLK, bytes_accessed=16 * tokens * channels, transcendentals=0
        ),
        name="mixer_heads",
    )(place, query, logits, value, margin, decay, gain.reshape(1, HEAD_CHANNELS), mine, other, partner)


def project_kernel(own_ref, left_ref, right_ref, far_ref, *refs):
    own_w, left_w, right_w, far_low_w, far_high_w, out_ref = refs
    width = 256

    def columns(c, _):
        cols = pl.ds(pl.multiple_of(c * width, width), width)
        total = jnp.zeros((out_ref.shape[0], width), F32)
        for h in range(own_ref.shape[0]):
            rows = columns_of(h)
            total += mm(own_ref[h], own_w[rows, cols], 1, 0)
            total += mm(left_ref[h], left_w[rows, cols], 1, 0)
            total += mm(right_ref[h], right_w[rows, cols], 1, 0)
            total += mm(far_ref[h], (far_low_w, far_high_w)[h][:, cols], 1, 0)
        out_ref[:, cols] = total.astype(BF16)
        return 0

    lax.fori_loop(0, out_ref.shape[1] // width, columns, 0)


def project(heads, weights):
    tokens, features = heads[0].shape[1], weights[0].shape[1]
    return pl.pallas_call(
        project_kernel,
        in_specs=[VMEM] * 9,
        out_specs=VMEM,
        out_shape=jax.ShapeDtypeStruct((tokens, features), BF16),
        cost_estimate=pl.CostEstimate(
            flops=8 * heads[0].size * features, bytes_accessed=8 * tokens * features, transcendentals=0
        ),
        name="mixer_project",
    )(*heads, *weights)


def slots_of(routes, core, experts):
    top_count, tokens = routes.shape
    number = lax.broadcasted_iota(jnp.int32, (experts, tokens), 0)
    named = [routes[k : k + 1, :] == number for k in range(top_count)]
    counts = sum(n.astype(F32) for n in named).astype(BF16)
    earlier = triangle_of(tokens, lambda r, c: r < c).astype(BF16)
    ranking = mm(counts, earlier, 1, 0)
    result = []
    for k, n in enumerate(named):
        slot = jnp.sum(jnp.where(n, ranking, 0.0), axis=0, keepdims=True).astype(jnp.int32)
        expert = routes[k : k + 1, :]
        chip = expert // 2
        far = jnp.where(expert - 2 * chip == core, 0, 1)
        late = slot >= TILE
        block = jnp.where(late, 2 + far, far)
        inside = jnp.where(late, slot - TILE + far * (TILE // 2), slot)
        result.append((block, chip * TILE + inside))
    return result


def dispatch_kernel(experts, core_ref, token_ref, gain_ref, route_ref, *refs):
    near_ref, others_ref, late_ref, normed_ref, chosen_ref = refs
    tokens = token_ref[...].astype(F32)
    scale = lax.rsqrt(jnp.mean(tokens * tokens, axis=-1, keepdims=True) + NORM_EPS)
    normed_ref[...] = (tokens * scale * gain_ref[...]).astype(BF16)
    rows = near_ref.shape[0]
    places = slots_of(route_ref[...], core_ref[0], experts)
    number = lax.broadcasted_iota(jnp.int32, chosen_ref.shape, 0)
    chosen_ref[...] = sum((b * rows + p == number).astype(F32) for b, p in places).astype(BF16)
    width = 512

    def columns(c, _):
        cols = pl.ds(pl.multiple_of(c * width, width), width)
        sent = mm(chosen_ref[...], normed_ref[:, cols], 1, 0).astype(BF16)
        near_ref[:, cols] = sent[:rows]
        others_ref[:rows, cols] = sent[rows : 2 * rows]
        late_ref[:, cols] = sent[2 * rows : 3 * rows]
        others_ref[rows:, cols] = sent[3 * rows :]
        return 0

    lax.fori_loop(0, near_ref.shape[1] // width, columns, 0)


def dispatch(core, tokens, gain, routes, experts):
    rows = experts // 2 * TILE
    count, features = tokens.shape
    return pl.pallas_call(
        functools.partial(dispatch_kernel, experts),
        in_specs=[SMEM, VMEM, VMEM, VMEM],
        out_specs=[VMEM] * 3,
        out_shape=[jax.ShapeDtypeStruct((n * rows, features), BF16) for n in (1, 2, 1)],
        scratch_shapes=[pltpu.VMEM((count, features), BF16), pltpu.VMEM((4 * rows, count), BF16)],
        cost_estimate=pl.CostEstimate(
            flops=8 * tokens.size * rows, bytes_accessed=10 * tokens.size, transcendentals=0
        ),
        name="dispatch_rows",
    )(core, tokens, gain.reshape(1, -1), routes)


def combine_kernel(experts, first, core_ref, weight_ref, route_ref, *refs):
    back_refs, out_ref = refs[:-1], refs[-1]
    if first:
        base_ref, back_refs = back_refs[0], back_refs[1:]
    weights = weight_ref[...]
    tokens = weights.shape[1]
    places = slots_of(route_ref[...], core_ref[0], experts)
    parts = []
    for block, ref in enumerate(back_refs, first):
        rows = ref.shape[0]
        number = lax.broadcasted_iota(jnp.int32, (rows, tokens), 0) + block * rows
        mixed = sum(
            jnp.where(b * rows + p == number, weights[k : k + 1, :], 0.0)
            for k, (b, p) in enumerate(places)
        )
        high = mixed.astype(BF16)
        parts += [(high, ref), ((mixed - high.astype(F32)).astype(BF16), ref)]
    width = 512

    def columns(c, _):
        cols = pl.ds(pl.multiple_of(c * width, width), width)
        total = base_ref[:, cols] if first else 0.0
        for mixed, ref in parts:
            total = total + mm(mixed, ref[:, cols], 0, 0)
        out_ref[:, cols] = total.astype(out_ref.dtype)
        return 0

    lax.fori_loop(0, out_ref.shape[1] // width, columns, 0)


def combine(core, weights, routes, experts, returned, first=0, base=()):
    tokens = routes.shape[1]
    rows, features = returned[0].shape
    return pl.pallas_call(
        functools.partial(combine_kernel, experts, first),
        in_specs=[SMEM] + [VMEM] * (2 + len(base) + len(returned)),
        out_specs=VMEM,
        out_shape=jax.ShapeDtypeStruct((tokens, features), BF16 if first else F32),
        cost_estimate=pl.CostEstimate(
            flops=16 * tokens * rows * features, bytes_accessed=10 * rows * features, transcendentals=0
        ),
        name="combine_rows",
    )(core, weights, routes, *base, *returned)


def clamped_unit(gate_pre, up_pre):
    gate_pre = jnp.minimum(gate_pre, CLAMP_LIMIT)
    up_pre = jnp.clip(up_pre, -CLAMP_LIMIT, CLAMP_LIMIT)
    return (up_pre + 1.0) * gate_pre * jax.nn.sigmoid(SIGMOID_SCALE * gate_pre)


def expert_kernel(pieces, me_ref, gate_ref, up_ref, down_ref, *refs):
    row_refs, out_refs, rows_ref, total_ref = refs[:pieces], refs[pieces:-2], refs[-2], refs[-1]
    step = pl.program_id(0)

    @pl.when(step == 0)
    def _():
        start = 0
        for ref in row_refs:
            rows_ref[start : start + ref.shape[0], :] = ref[...]
            start += ref.shape[0]
        total_ref[...] = jnp.zeros_like(total_ref)

    rows = rows_ref[...]
    gate_pre = mm(rows, gate_ref[...], 1, 0)
    up_pre = mm(rows, up_ref[...], 1, 0)
    hidden = clamped_unit(gate_pre, up_pre).astype(BF16)
    part = 512

    def columns(c, _):
        cols = pl.ds(pl.multiple_of(c * part, part), part)
        total_ref[:, cols] += mm(hidden, down_ref[:, cols], 1, 0)
        return 0

    lax.fori_loop(0, total_ref.shape[1] // part, columns, 0)

    @pl.when(step == pl.num_programs(0) - 1)
    def _():
        if len(out_refs) > 1:
            start = 0
            for ref in out_refs:
                ref[...] = total_ref[start : start + ref.shape[0], :].astype(BF16)
                start += ref.shape[0]
        else:
            (ref,) = out_refs
            owners, per = ref.shape[0], ref.shape[1]
            for k, by in enumerate((0, owners - 1, 1, 2)):
                owner = lax.rem(me_ref[0] + by, owners)
                ref[owner] = total_ref[k * per : (k + 1) * per, :].astype(BF16)


def expert_parts(me, pieces, gate_weight, up_weight, down_weight, owners=None):
    features, hidden = gate_weight.shape
    width = min(256, hidden)
    rows = sum(p.shape[0] for p in pieces)
    whole = [pl.BlockSpec(p.shape, lambda f: (0, 0)) for p in pieces]
    out_specs, out_shape = whole, [jax.ShapeDtypeStruct(p.shape, BF16) for p in pieces]
    if owners:
        by_owner = (owners, rows // owners, features)
        out_specs = [pl.BlockSpec(by_owner, lambda f: (0, 0, 0))]
        out_shape = [jax.ShapeDtypeStruct(by_owner, BF16)]
    return pl.pallas_call(
        functools.partial(expert_kernel, len(pieces)),
        grid=(hidden // width,),
        in_specs=[
            SMEM,
            pl.BlockSpec((features, width), lambda f: (0, f)),
            pl.BlockSpec((features, width), lambda f: (0, f)),
            pl.BlockSpec((width, features), lambda f: (f, 0)),
            *whole,
        ],
        out_specs=out_specs,
        out_shape=out_shape,
        scratch_shapes=[pltpu.VMEM((rows, features), BF16), pltpu.VMEM((rows, features), F32)],
        cost_estimate=pl.CostEstimate(
            flops=6 * rows * features * hidden,
            bytes_accessed=6 * features * hidden + 4 * rows * features,
            transcendentals=0,
        ),
        name="expert_parts",
    )(me, gate_weight, up_weight, down_weight, *pieces)


def turned(x, axis, by):
    size = lax.axis_size(axis)
    return lax.ppermute(x, axis, [(i, (i + by) % size) for i in range(size)])


def gathered_pieces(own):
    half = own.shape[0] // 2
    left = turned(own, "tp", 1)
    right = turned(own, "tp", -1)
    far_low = turned(left[:half], "tp", 1)
    far_high = turned(right[half:], "tp", -1)
    return own, left, right, far_low, far_high


def summed_pieces(parts):
    own, left, right, far_low, far_high = parts
    half = own.shape[0] // 2
    from_right = turned(far_low, "tp", -1)
    from_left = turned(far_high, "tp", 1)
    low = (left[:half].astype(F32) + from_right.astype(F32)).astype(BF16)
    high = (right[half:].astype(F32) + from_left.astype(F32)).astype(BF16)
    to_left = jnp.concatenate([low, left[half:]], axis=0)
    to_right = jnp.concatenate([right[:half], high], axis=0)
    back_right = turned(to_left, "tp", -1)
    back_left = turned(to_right, "tp", 1)
    return (own.astype(F32) + back_left.astype(F32) + back_right.astype(F32)).astype(BF16)


def sent_over_chips(rows, chips):
    blocks = rows.reshape(chips, -1, rows.shape[1])
    return lax.all_to_all(blocks, "ep_0", split_axis=0, concat_axis=0, tiled=True).reshape(rows.shape)


def after(value, earlier):
    return lax.optimization_barrier((value, earlier))[0]


def body(
    query,
    forget_gate_logits,
    value,
    forget_lower_margin,
    position_log_decay,
    head_norm_gain,
    mixer_output_weight,
    second_batch_tokens,
    expert_norm_gain,
    routes,
    chosen_expert_weight,
    gate_weight,
    up_weight,
    down_weight,
):
    n_ep = lax.axis_size(EP)
    chips = lax.axis_size("ep_0")
    owners = lax.axis_size("tp")
    core = lax.axis_index("ep_1").astype(jnp.int32).reshape(1)
    chip = lax.axis_index("ep_0").astype(jnp.int32).reshape(1)
    me = lax.axis_index("tp").astype(jnp.int32).reshape(1)
    place = jnp.stack([core[0], lax.axis_index("tp").astype(jnp.int32)])

    weights_all = gathered_pieces(mixer_output_weight)

    routes_t, weights_t = jnp.transpose(routes), jnp.transpose(chosen_expert_weight)
    near, others, late_near = dispatch(core, second_batch_tokens, expert_norm_gain, routes_t, n_ep)
    others = turned(others, "ep_1", 1)
    far, late = others[: near.shape[0]], late_near + others[near.shape[0] :]

    state = mixer_states(
        forget_gate_logits, value, forget_lower_margin, position_log_decay
    )
    partner = turned(state, "ep_1", 1)
    chip_state = merged_states(core, state, partner)
    gathered = lax.all_gather(chip_state, "ep_0", axis=0, tiled=False)

    sums = []
    arrived = None
    for c, rows in enumerate((near, far, late)):
        if arrived is not None:
            rows = after(rows, (arrived, late))
        arrived = sent_over_chips(rows, chips)
        pieces = gathered_pieces(arrived)
        if not c:
            pieces = after(pieces, weights_all)
        parts = expert_parts(
            me,
            pieces,
            gate_weight[0],
            up_weight[0],
            down_weight[0],
            owners if c else None,
        )
        if c:
            parts = parts[0].reshape(owners * rows.shape[0], -1)
            sums.append(lax.psum_scatter(parts, "tp", scatter_dimension=0, tiled=True))
        else:
            sums.append(summed_pieces(parts))

    returned = []
    for rows in sums:
        rows = after(rows, returned[-1] if returned else arrived)
        returned.append(sent_over_chips(rows, chips))

    entering_mine = entering_states(chip, gathered)
    entering_other = turned(entering_mine, "ep_1", 1)
    heads = mixer_heads(
        place,
        query,
        forget_gate_logits,
        value,
        forget_lower_margin,
        position_log_decay,
        head_norm_gain,
        entering_mine,
        entering_other,
        partner,
        owners,
    )
    heads = (
        heads[0],
        turned(heads[1], "tp", 1),
        turned(heads[owners - 1], "tp", -1),
        turned(heads[2], "tp", 2),
    )
    first_mixer_output = project(heads, weights_all)

    back_near, back_far, back_late = returned
    base = combine(core, weights_t, routes_t, n_ep, (back_near, turned(back_far, "ep_1", 1)))
    moe_out = combine(
        core,
        weights_t,
        routes_t,
        n_ep,
        (back_late, turned(back_late, "ep_1", 1)),
        2,
        (base,),
    )
    return (first_mixer_output, moe_out)


def solution(mesh):
    cores = 2
    finer = Mesh(
        mesh.devices.reshape(mesh.shape["grp"], mesh.shape["ep"] // cores, cores, mesh.shape["tp"]),
        ("grp", "ep_0", "ep_1", "tp"),
    )
    placed = (
        P(GRP_EP, "tp"),
        P(GRP_EP, "tp"),
        P(GRP_EP, "tp"),
        P(None, "tp"),
        P("tp", GRP_EP),
        P(),
        P("tp", None),
        P(GRP_EP_TP, None),
        P(),
        P(GRP_EP_TP, None),
        P(GRP_EP_TP, None),
        P(EP, None, "tp"),
        P(EP, None, "tp"),
        P(EP, "tp", None),
    )
    return jax.shard_map(
        body,
        mesh=finer,
        in_specs=placed,
        out_specs=(P(GRP_EP_TP, None), P(GRP_EP_TP, None)),
        check_vma=False,
    )
```

```python
import functools

import jax
import jax.numpy as jnp
from jax import lax
from jax.experimental import pallas as pl
from jax.experimental.pallas import tpu as pltpu
from jax.sharding import Mesh
from jax.sharding import PartitionSpec as P


HEAD_CHANNELS = 128
BLK = 128
STATE_ROWS = HEAD_CHANNELS + 16
EP = ("ep_0", "ep_1")
GRP_EP = ("grp", "ep_0", "ep_1")
GRP_EP_TP = ("grp", "ep_0", "ep_1", "tp")
TILE = 8
STRIP = 32

NORM_EPS = 1e-06
CLAMP_LIMIT = 7.0
SIGMOID_SCALE = 1.702

F32 = jnp.float32
BF16 = jnp.bfloat16
SMEM = pl.BlockSpec(memory_space=pltpu.SMEM)
VMEM = pl.BlockSpec(memory_space=pltpu.VMEM)


def mm(a, b, lhs_dim, rhs_dim):
    return lax.dot_general(
        a, b, (((lhs_dim,), (rhs_dim,)), ((), ())), preferred_element_type=F32
    )


def pieces_of(x):
    high = x.astype(BF16)
    rest = x - high.astype(F32)
    middle = rest.astype(BF16)
    low = (rest - middle.astype(F32)).astype(BF16)
    return high, middle, low


def summed_along(triangle, x):
    return sum(mm(triangle, piece, 1, 0) for piece in pieces_of(x))


def triangle_of(size, keep):
    rows = lax.broadcasted_iota(jnp.int32, (size, size), 0)
    columns = lax.broadcasted_iota(jnp.int32, (size, size), 1)
    return keep(rows, columns)


def block_gates(logits, margin, decay_row, triangle):
    closing = jnp.exp(margin) * jax.nn.sigmoid(-logits.astype(F32))
    spikes = jnp.transpose(jnp.broadcast_to(decay_row, (BLK, BLK)))
    return closing, summed_along(triangle, jnp.log1p(-closing) + spikes)


def advanced(state, total, closing, cumul, values):
    key_state = (closing * jnp.exp(total - cumul)).astype(BF16)
    return state * jnp.exp(total) + mm(values, key_state, 0, 0)


def rows_of(block):
    return pl.ds(pl.multiple_of(block * BLK, BLK), BLK)


def columns_of(head):
    return slice(head * HEAD_CHANNELS, (head + 1) * HEAD_CHANNELS)


def states_kernel(logits_ref, value_ref, margin_ref, decay_ref, state_ref):
    blocks = logits_ref.shape[0] // BLK
    heads = state_ref.shape[0]
    triangles = (
        triangle_of(BLK, lambda r, c: r >= c).astype(BF16),
        triangle_of(BLK, lambda r, c: r <= c).astype(BF16),
    )
    chains = [(h, d) for h in range(heads) for d in range(2)]

    def step(i, carry):
        after = []
        for (h, d), (state, log) in zip(chains, carry):
            rows = rows_of(i if d == 0 else blocks - 1 - i)
            closing, cumul = block_gates(
                logits_ref[rows, columns_of(h)],
                margin_ref[d : d + 1, columns_of(h)],
                decay_ref[h : h + 1, rows],
                triangles[d],
            )
            total = cumul[BLK - 1 :, :] if d == 0 else cumul[:1, :]
            state = advanced(state, total, closing, cumul, value_ref[rows, columns_of(h)])
            after.append((state, log + total))
        return tuple(after)

    zero = (jnp.zeros((HEAD_CHANNELS, HEAD_CHANNELS), F32), jnp.zeros((1, HEAD_CHANNELS), F32))
    for (h, d), (state, log) in zip(
        chains, lax.fori_loop(0, blocks, step, (zero,) * len(chains))
    ):
        store_state(state_ref, (h, d), state, log)


def mixer_states(logits, value, margin, decay):
    tokens, channels = logits.shape
    heads = channels // HEAD_CHANNELS
    return pl.pallas_call(
        states_kernel,
        in_specs=[VMEM] * 4,
        out_specs=VMEM,
        out_shape=jax.ShapeDtypeStruct((heads, 2, STATE_ROWS, HEAD_CHANNELS), BF16),
        cost_estimate=pl.CostEstimate(
            flops=24 * tokens * channels * BLK, bytes_accessed=5 * tokens * channels, transcendentals=0
        ),
        name="mixer_states",
    )(logits, value, margin, decay)


def decay_of(block):
    tail = block[HEAD_CHANNELS:, :].astype(F32)
    return tail[0:1, :] + tail[1:2, :] + tail[2:3, :]


def store_state(ref, index, state, log):
    places = lax.broadcasted_iota(jnp.int32, (STATE_ROWS - HEAD_CHANNELS, HEAD_CHANNELS), 0)
    tail = jnp.zeros(places.shape, F32)
    for k, piece in enumerate(pieces_of(log)):
        tail = jnp.where(places == k, piece.astype(F32), tail)
    ref[(*index, slice(0, HEAD_CHANNELS), slice(None))] = state.astype(BF16)
    ref[(*index, slice(HEAD_CHANNELS, STATE_ROWS), slice(None))] = tail.astype(BF16)


def merge_kernel(core_ref, own_ref, partner_ref, chip_ref):
    core = core_ref[0]
    for d in range(2):
        own, partner = own_ref[core, d], partner_ref[core, d]
        own_last = (core == 1) if d == 0 else (core == 0)
        first = jnp.where(own_last, partner.astype(F32), own.astype(F32))
        second = jnp.where(own_last, own.astype(F32), partner.astype(F32))
        state = first[:HEAD_CHANNELS] * jnp.exp(decay_of(second)) + second[:HEAD_CHANNELS]
        store_state(chip_ref, (d,), state, decay_of(first) + decay_of(second))


def merged_states(core, own, partner):
    return pl.pallas_call(
        merge_kernel,
        in_specs=[SMEM, VMEM, VMEM],
        out_specs=VMEM,
        out_shape=jax.ShapeDtypeStruct(own.shape[1:], BF16),
        cost_estimate=pl.CostEstimate(flops=8 * own.size, bytes_accessed=5 * own.size, transcendentals=0),
        name="mixer_merge",
    )(core, own, partner)


def entering_kernel(chip_ref, gathered_ref, out_ref):
    chips = gathered_ref.shape[0]
    chip = chip_ref[0]
    for d in range(2):

        def step(i, state):
            j = i if d == 0 else chips - 1 - i
            passed = (j < chip) if d == 0 else (j > chip)
            block = gathered_ref[j, d]
            later = state * jnp.exp(decay_of(block)) + block[:HEAD_CHANNELS, :].astype(F32)
            return jnp.where(passed, later, state)

        zero = jnp.zeros((HEAD_CHANNELS, HEAD_CHANNELS), F32)
        out_ref[d] = lax.fori_loop(0, chips, step, zero).astype(BF16)


def entering_states(chip, gathered):
    return pl.pallas_call(
        entering_kernel,
        in_specs=[SMEM, VMEM],
        out_specs=VMEM,
        out_shape=jax.ShapeDtypeStruct((2, HEAD_CHANNELS, HEAD_CHANNELS), BF16),
        cost_estimate=pl.CostEstimate(
            flops=8 * gathered.size, bytes_accessed=2 * gathered.size, transcendentals=0
        ),
        name="mixer_entering",
    )(chip, gathered)


def heads_kernel(
    place_ref,
    query_ref,
    logits_ref,
    value_ref,
    margin_ref,
    decay_ref,
    gain_ref,
    mine_ref,
    other_ref,
    partner_ref,
    out_ref,
    part_ref,
):
    blocks = logits_ref.shape[0] // BLK
    owners, heads = out_ref.shape[0], out_ref.shape[1]
    per = out_ref.shape[2] // BLK
    core, me = place_ref[0], place_ref[1]
    chains = [(h, d) for h in range(heads) for d in range(2)]

    def entering(h, d):
        state = jnp.where(core == h, mine_ref[d].astype(F32), other_ref[d].astype(F32))
        block = partner_ref[h, d]
        later = state * jnp.exp(decay_of(block)) + block[:HEAD_CHANNELS, :].astype(F32)
        return jnp.where((core == 1) if d == 0 else (core == 0), later, state)

    def part(block, state, h, d):
        rows = rows_of(block)
        keep = triangle_of(BLK, (lambda r, c: r >= c) if d == 0 else (lambda r, c: r <= c))
        values = value_ref[rows, columns_of(h)]
        closing, cumul = block_gates(
            logits_ref[rows, columns_of(h)],
            margin_ref[d : d + 1, columns_of(h)],
            decay_ref[h : h + 1, rows],
            keep.astype(BF16),
        )
        queries = query_ref[rows, columns_of(h)].astype(F32)
        queries = queries * jax.nn.sigmoid(queries) * HEAD_CHANNELS ** (-0.5)
        query_in = (queries * jnp.exp(cumul)).astype(BF16)
        key_in = (closing * jnp.exp(-cumul)).astype(BF16)
        scores = jnp.where(keep, mm(query_in, key_in, 1, 1), 0.0).astype(BF16)
        part_ref[d, rows, columns_of(h)] = mm(scores, values, 1, 0) + mm(
            query_in, state.astype(BF16), 1, 1
        )
        total = cumul[BLK - 1 :, :] if d == 0 else cumul[:1, :]
        return advanced(state, total, closing, cumul, values)

    def step(i, states):
        return tuple(
            part(i if d == 0 else blocks - 1 - i, state, h, d)
            for (h, d), state in zip(chains, states)
        )

    lax.fori_loop(0, blocks, step, tuple(entering(h, d) for h, d in chains))

    def finish(block, _):
        rows = rows_of(block)
        away = lax.rem(block // per - me + owners, owners)
        part_rows = pl.ds(pl.multiple_of((block % per) * BLK, BLK), BLK)
        for h in range(heads):
            mix = part_ref[0, rows, columns_of(h)] + part_ref[1, rows, columns_of(h)]
            scale = lax.rsqrt(jnp.mean(mix * mix, axis=-1, keepdims=True) + NORM_EPS)
            out_ref[away, h, part_rows, :] = (mix * scale * gain_ref[...]).astype(BF16)
        return 0

    lax.fori_loop(0, blocks, finish, 0)


def mixer_heads(place, query, logits, value, margin, decay, gain, mine, other, partner, owners):
    tokens, channels = logits.shape
    heads = channels // HEAD_CHANNELS
    return pl.pallas_call(
        heads_kernel,
        in_specs=[SMEM] + [VMEM] * 9,
        out_specs=VMEM,
        scratch_shapes=[pltpu.VMEM((2, tokens, channels), F32)],
        out_shape=jax.ShapeDtypeStruct((owners, heads, tokens // owners, HEAD_CHANNELS), BF16),
        cost_estimate=pl.CostEstimate(
            flops=48 * tokens * channels * BLK, bytes_accessed=16 * tokens * channels, transcendentals=0
        ),
        name="mixer_heads",
    )(place, query, logits, value, margin, decay, gain.reshape(1, HEAD_CHANNELS), mine, other, partner)


def project_kernel(core_ref, own_ref, left_ref, right_ref, far_ref, weight_ref, mine_ref, other_ref, out_ref):
    core = core_ref[0]
    width = 256

    def columns(c, _):
        cols = pl.ds(pl.multiple_of(c * width, width), width)
        total = jnp.zeros((out_ref.shape[0], width), F32)
        for h, (which, ref) in enumerate(((core, mine_ref), (1 - core, other_ref))):
            total += mm(own_ref[h], weight_ref[columns_of(h), cols], 1, 0)
            for k, heads_ref in enumerate((left_ref, right_ref, far_ref)):
                total += mm(heads_ref[which], ref[columns_of(k), cols], 1, 0)
        out_ref[:, cols] = total.astype(BF16)
        return 0

    lax.fori_loop(0, out_ref.shape[1] // width, columns, 0)


def project(core, heads, weight, mine, other):
    tokens, features = heads[0].shape[1], weight.shape[1]
    return pl.pallas_call(
        project_kernel,
        in_specs=[SMEM] + [VMEM] * 7,
        out_specs=VMEM,
        out_shape=jax.ShapeDtypeStruct((tokens, features), BF16),
        cost_estimate=pl.CostEstimate(
            flops=8 * heads[0].size * features, bytes_accessed=8 * tokens * features, transcendentals=0
        ),
        name="mixer_project",
    )(core, *heads, weight, mine, other)


def slots_of(routes, core, experts):
    top_count, tokens = routes.shape
    number = lax.broadcasted_iota(jnp.int32, (experts, tokens), 0)
    named = [routes[k : k + 1, :] == number for k in range(top_count)]
    counts = sum(n.astype(F32) for n in named).astype(BF16)
    earlier = triangle_of(tokens, lambda r, c: r < c).astype(BF16)
    ranking = mm(counts, earlier, 1, 0)
    result = []
    for k, n in enumerate(named):
        slot = jnp.sum(jnp.where(n, ranking, 0.0), axis=0, keepdims=True).astype(jnp.int32)
        expert = routes[k : k + 1, :]
        chip = expert // 2
        far = jnp.where(expert - 2 * chip == core, 0, 1)
        late = slot >= TILE
        block = jnp.where(late, 2 + far, far)
        inside = jnp.where(late, slot - TILE + far * (TILE // 2), slot)
        result.append((block, chip * TILE + inside))
    return result


def dispatch_kernel(experts, core_ref, token_ref, gain_ref, route_ref, near_ref, others_ref, late_ref):
    tokens = token_ref[...].astype(F32)
    scale = lax.rsqrt(jnp.mean(tokens * tokens, axis=-1, keepdims=True) + NORM_EPS)
    normed = (tokens * scale * gain_ref[...]).astype(BF16)
    rows = near_ref.shape[0]
    places = slots_of(route_ref[...], core_ref[0], experts)
    targets = ((near_ref, 0), (others_ref, 0), (late_ref, 0), (others_ref, rows))
    for block, (ref, start) in enumerate(targets):
        number = lax.broadcasted_iota(jnp.int32, (rows, tokens.shape[0]), 0) + block * rows
        chosen = sum((b * rows + p == number).astype(F32) for b, p in places)
        ref[start : start + rows, :] = mm(chosen.astype(BF16), normed, 1, 0).astype(BF16)


def dispatch(core, tokens, gain, routes, experts):
    rows = experts // 2 * TILE
    return pl.pallas_call(
        functools.partial(dispatch_kernel, experts),
        in_specs=[SMEM, VMEM, VMEM, VMEM],
        out_specs=[VMEM] * 3,
        out_shape=[jax.ShapeDtypeStruct((n * rows, tokens.shape[1]), BF16) for n in (1, 2, 1)],
        cost_estimate=pl.CostEstimate(
            flops=8 * tokens.size * rows, bytes_accessed=10 * tokens.size, transcendentals=0
        ),
        name="dispatch_rows",
    )(core, tokens, gain.reshape(1, -1), routes)


def combine_kernel(experts, first, core_ref, weight_ref, route_ref, *refs):
    back_refs, out_ref = refs[:-1], refs[-1]
    if first:
        base_ref, back_refs = back_refs[0], back_refs[1:]
    weights = weight_ref[...]
    tokens = weights.shape[1]
    places = slots_of(route_ref[...], core_ref[0], experts)
    total = base_ref[...] if first else 0.0
    for block, ref in enumerate(back_refs, first):
        rows = ref.shape[0]
        number = lax.broadcasted_iota(jnp.int32, (rows, tokens), 0) + block * rows
        mixed = sum(
            jnp.where(b * rows + p == number, weights[k : k + 1, :], 0.0)
            for k, (b, p) in enumerate(places)
        )
        high = mixed.astype(BF16)
        low = (mixed - high.astype(F32)).astype(BF16)
        total = total + (mm(high, ref[...], 0, 0) + mm(low, ref[...], 0, 0))
    out_ref[...] = total.astype(out_ref.dtype)


def combine(core, weights, routes, experts, returned, first=0, base=()):
    tokens = routes.shape[1]
    rows, features = returned[0].shape
    return pl.pallas_call(
        functools.partial(combine_kernel, experts, first),
        in_specs=[SMEM] + [VMEM] * (2 + len(base) + len(returned)),
        out_specs=VMEM,
        out_shape=jax.ShapeDtypeStruct((tokens, features), BF16 if first else F32),
        cost_estimate=pl.CostEstimate(
            flops=16 * tokens * rows * features, bytes_accessed=10 * rows * features, transcendentals=0
        ),
        name="combine_rows",
    )(core, weights, routes, *base, *returned)


def clamped_unit(gate_pre, up_pre):
    gate_pre = jnp.minimum(gate_pre, CLAMP_LIMIT)
    up_pre = jnp.clip(up_pre, -CLAMP_LIMIT, CLAMP_LIMIT)
    return (up_pre + 1.0) * gate_pre * jax.nn.sigmoid(SIGMOID_SCALE * gate_pre)


def strip_of(start, i):
    return pl.ds(pl.multiple_of(start + i * STRIP, STRIP), STRIP)


def copied(to_ref, to_start, from_ref, from_start, rows):
    def step(i, _):
        strip = from_ref[strip_of(from_start, i), :]
        to_ref[strip_of(to_start, i), :] = strip.astype(to_ref.dtype)
        return 0

    lax.fori_loop(0, rows // STRIP, step, 0)


def expert_kernel(pieces, me_ref, gate_ref, up_ref, down_ref, *refs):
    row_refs, (out_ref, rows_ref, total_ref) = refs[:pieces], refs[pieces:]
    step = pl.program_id(0)

    @pl.when(step == 0)
    def _():
        start = 0
        for ref in row_refs:
            copied(rows_ref, start, ref, 0, ref.shape[0])
            start += ref.shape[0]

        def cleared(i, _):
            total_ref[strip_of(0, i), :] = jnp.zeros((STRIP, total_ref.shape[1]), F32)
            return 0

        lax.fori_loop(0, total_ref.shape[0] // STRIP, cleared, 0)

    rows = rows_ref[...]
    gate_pre = mm(rows, gate_ref[...], 1, 0)
    up_pre = mm(rows, up_ref[...], 1, 0)
    hidden = clamped_unit(gate_pre, up_pre).astype(BF16)
    total_ref[...] += mm(hidden, down_ref[...], 1, 0)

    @pl.when(step == pl.num_programs(0) - 1)
    def _():
        owners, per = out_ref.shape[0], out_ref.shape[1]
        for k, by in enumerate((0, owners - 1, 1, 2)):
            owner = lax.rem(me_ref[0] + by, owners)
            copied(out_ref.at[owner], 0, total_ref, k * per, per)


def expert_parts(me, pieces, gate_weight, up_weight, down_weight, owners):
    features, hidden = gate_weight.shape
    width = min(256, hidden)
    rows = sum(p.shape[0] for p in pieces)
    whole = [pl.BlockSpec(p.shape, lambda f: (0, 0)) for p in pieces]
    by_owner = (owners, rows // owners, features)
    return pl.pallas_call(
        functools.partial(expert_kernel, len(pieces)),
        grid=(hidden // width,),
        in_specs=[
            SMEM,
            pl.BlockSpec((features, width), lambda f: (0, f)),
            pl.BlockSpec((features, width), lambda f: (0, f)),
            pl.BlockSpec((width, features), lambda f: (f, 0)),
            *whole,
        ],
        out_specs=pl.BlockSpec(by_owner, lambda f: (0, 0, 0)),
        out_shape=jax.ShapeDtypeStruct(by_owner, BF16),
        scratch_shapes=[pltpu.VMEM((rows, features), BF16), pltpu.VMEM((rows, features), F32)],
        cost_estimate=pl.CostEstimate(
            flops=6 * rows * features * hidden,
            bytes_accessed=6 * features * hidden + 4 * rows * features,
            transcendentals=0,
        ),
        name="expert_parts",
    )(me, gate_weight, up_weight, down_weight, *pieces)


def turned(x, axis, by):
    size = lax.axis_size(axis)
    return lax.ppermute(x, axis, [(i, (i + by) % size) for i in range(size)])


def gathered_pieces(own):
    half = own.shape[0] // 2
    left = turned(own, "tp", 1)
    right = turned(own, "tp", -1)
    far_low = turned(left[:half], "tp", 1)
    far_high = turned(right[half:], "tp", -1)
    return own, left, right, far_low, far_high


def summed_pieces(parts, me, owners):
    half = parts.shape[1] // 2

    def rows_for(by, start=0, count=2 * half):
        owner = lax.rem(me + by, owners)
        return lax.dynamic_slice(parts, (owner, start, 0), (1, count, parts.shape[2]))[0]

    own, left, right = rows_for(0), rows_for(owners - 1), rows_for(1)
    far_low, far_high = rows_for(2, 0, half), rows_for(2, half, half)
    from_right = turned(far_low, "tp", -1)
    from_left = turned(far_high, "tp", 1)
    low = (left[:half].astype(F32) + from_right.astype(F32)).astype(BF16)
    high = (right[half:].astype(F32) + from_left.astype(F32)).astype(BF16)
    to_left = jnp.concatenate([low, left[half:]], axis=0)
    to_right = jnp.concatenate([right[:half], high], axis=0)
    back_right = turned(to_left, "tp", -1)
    back_left = turned(to_right, "tp", 1)
    return (own.astype(F32) + back_left.astype(F32) + back_right.astype(F32)).astype(BF16)


def sent_over_chips(rows, chips):
    blocks = rows.reshape(chips, -1, rows.shape[1])
    return lax.all_to_all(blocks, "ep_0", split_axis=0, concat_axis=0, tiled=True).reshape(rows.shape)


def after(value, earlier):
    return lax.optimization_barrier((value, earlier))[0]


def body(
    query,
    forget_gate_logits,
    value,
    forget_lower_margin,
    position_log_decay,
    head_norm_gain,
    mixer_output_weight,
    second_batch_tokens,
    expert_norm_gain,
    routes,
    chosen_expert_weight,
    gate_weight,
    up_weight,
    down_weight,
):
    n_ep = lax.axis_size(EP)
    chips = lax.axis_size("ep_0")
    owners = lax.axis_size("tp")
    core = lax.axis_index("ep_1").astype(jnp.int32).reshape(1)
    chip = lax.axis_index("ep_0").astype(jnp.int32).reshape(1)
    me = lax.axis_index("tp").astype(jnp.int32).reshape(1)
    place = jnp.stack([core[0], lax.axis_index("tp").astype(jnp.int32)])

    half = mixer_output_weight.shape[0] // 2
    weight_part = lax.dynamic_slice_in_dim(mixer_output_weight, core[0] * half, half, 0)
    weight_left = turned(weight_part, "tp", 1)
    weight_right = turned(weight_part, "tp", -1)
    weight_far = turned(weight_left, "tp", 1)
    weight_mine = jnp.concatenate((weight_left, weight_right, weight_far), axis=0)
    weight_other = turned(weight_mine, "ep_1", 1)

    routes_t, weights_t = jnp.transpose(routes), jnp.transpose(chosen_expert_weight)
    near, others, late_near = dispatch(core, second_batch_tokens, expert_norm_gain, routes_t, n_ep)
    others = turned(others, "ep_1", 1)
    far, late = others[: near.shape[0]], late_near + others[near.shape[0] :]

    state = mixer_states(
        forget_gate_logits, value, forget_lower_margin, position_log_decay
    )
    partner = turned(state, "ep_1", 1)
    chip_state = merged_states(core, state, partner)
    gathered = lax.all_gather(chip_state, "ep_0", axis=0, tiled=False)

    sums = []
    arrived = None
    for c, rows in enumerate((near, far, late)):
        if arrived is not None:
            rows = after(rows, (arrived, late))
        arrived = sent_over_chips(rows, chips)
        pieces = gathered_pieces(arrived)
        parts = expert_parts(me, pieces, gate_weight[0], up_weight[0], down_weight[0], owners)
        if c:
            parts = parts.reshape(owners * rows.shape[0], -1)
            sums.append(lax.psum_scatter(parts, "tp", scatter_dimension=0, tiled=True))
        else:
            sums.append(summed_pieces(parts, me[0], owners))

    returned = []
    for rows in sums:
        rows = after(rows, returned[-1] if returned else arrived)
        returned.append(sent_over_chips(rows, chips))

    entering_mine = entering_states(chip, gathered)
    entering_other = turned(entering_mine, "ep_1", 1)
    heads = mixer_heads(
        place,
        query,
        forget_gate_logits,
        value,
        forget_lower_margin,
        position_log_decay,
        head_norm_gain,
        entering_mine,
        entering_other,
        partner,
        owners,
    )
    heads = (
        heads[0],
        turned(heads[1], "tp", 1),
        turned(heads[owners - 1], "tp", -1),
        turned(heads[2], "tp", 2),
    )
    first_mixer_output = project(core, heads, mixer_output_weight, weight_mine, weight_other)

    back_near, back_far, back_late = returned
    base = combine(core, weights_t, routes_t, n_ep, (back_near, turned(back_far, "ep_1", 1)))
    moe_out = combine(
        core,
        weights_t,
        routes_t,
        n_ep,
        (back_late, turned(back_late, "ep_1", 1)),
        2,
        (base,),
    )
    return (first_mixer_output, moe_out)


def solution(mesh):
    cores = 2
    finer = Mesh(
        mesh.devices.reshape(mesh.shape["grp"], mesh.shape["ep"] // cores, cores, mesh.shape["tp"]),
        ("grp", "ep_0", "ep_1", "tp"),
    )
    placed = (
        P(GRP_EP, "tp"),
        P(GRP_EP, "tp"),
        P(GRP_EP, "tp"),
        P(None, "tp"),
        P("tp", GRP_EP),
        P(),
        P("tp", None),
        P(GRP_EP_TP, None),
        P(),
        P(GRP_EP_TP, None),
        P(GRP_EP_TP, None),
        P(EP, None, "tp"),
        P(EP, None, "tp"),
        P(EP, "tp", None),
    )
    return jax.shard_map(
        body,
        mesh=finer,
        in_specs=placed,
        out_specs=(P(GRP_EP_TP, None), P(GRP_EP_TP, None)),
        check_vma=False,
    )
```
